128 devices in a mesh: sp: 16 (over z, y), tp: 8 (over x, core).
Axes of the slice: x: 4, y: 4, z: 4, core: 2. Of those that a mesh axis runs over, the one named last changes fastest.
Arguments:
- queries: bfloat16 [16384, 1024], P('sp', 'tp'), may hold values from -6 to 6
- keys: bfloat16 [16384, 1024], P('sp', 'tp'), may hold values from -6 to 6
- values: bfloat16 [16384, 1024], P('sp', 'tp'), may hold values from -6 to 6
- stick_bias: bfloat16 [16384, 8], P('sp', 'tp'), may hold values from -14 to 0
- residual: bfloat16 [16384, 2048], P(('sp', 'tp')), may hold values from -6 to 6
- out_weight: bfloat16 [1024, 2048], replicated, may hold values from -0.1875 to 0.1875
- norm_gain: float32 [2048], replicated, may hold values from 0.1 to 1.9
- gate_weight: bfloat16 [2048, 5632], P('sp', 'tp'), may hold values from -0.125 to 0.125
- value_weight: bfloat16 [2048, 5632], P('sp', 'tp'), may hold values from -0.125 to 0.125
- down_weight: bfloat16 [2048, 5632], P('sp', 'tp'), may hold values from -0.078125 to 0.078125
- conv_gate: float32 [3, 5632], P(None, 'tp'), may hold values from -3.5 to 3.5
- conv_value: float32 [3, 5632], P(None, 'tp'), may hold values from -3.5 to 3.5
Outputs:
- mixed: bfloat16 [16384, 2048], P(('sp', 'tp'))
The draws below stay inside these ranges and needn't reach their ends.
All inputs are finite; a program needn't handle non-finite values.
Results may differ from the reference program's by a relative error of at most 0.023.
Values may be sent and summed in bfloat16 or wider, within the bound.
A program may use at most 128 MiB of HBM per device.

```python
import jax
import jax.numpy as jnp
from jax import lax

D = 2048
FOCUS_CHANNELS = 8
HEAD_DIM = 128
FF = 5632
WIDTH = 3
TOK_DEV = 1024
STRING_LENGTH = 16384
N_TP = 8


def draw_values(key, part):
    mean_key, noise_key = jax.random.split(jax.random.fold_in(key, 7), 2)
    blocks = STRING_LENGTH // TOK_DEV
    means = 0.3 * jnp.clip(jax.random.normal(mean_key, (blocks, FOCUS_CHANNELS * HEAD_DIM), jnp.float32), -4.0, 4.0)
    noise = jnp.clip(jax.random.normal(noise_key, (STRING_LENGTH, FOCUS_CHANNELS * HEAD_DIM), jnp.float32), -4.0, 4.0)
    return (jnp.repeat(means, TOK_DEV, axis=0) + noise).astype(jnp.bfloat16)


def draw_stick_bias(key, part):
    complete_lookup_line = jax.random.split(jax.random.fold_in(key, 11), 5)
    blocks = STRING_LENGTH // TOK_DEV
    slow_share = 0.5
    lagging_fraction = jax.random.uniform(complete_lookup_line[0], (FOCUS_CHANNELS,), jnp.float32) < slow_share
    base = jnp.where(lagging_fraction, jnp.log(0.6 / STRING_LENGTH) - 2.5, jnp.log(1.0 / 40.0) - 2.5)
    block_shift = jax.random.uniform(complete_lookup_line[1], (blocks, FOCUS_CHANNELS), jnp.float32, -0.7, 0.7)
    jitter = jnp.clip(2.0 * jax.random.normal(complete_lookup_line[2], (STRING_LENGTH, FOCUS_CHANNELS), jnp.float32), -5.0, 5.0)
    spike_location = jax.random.randint(complete_lookup_line[3], (3,), 0, STRING_LENGTH)
    spike_displacement_jitter = jax.random.uniform(complete_lookup_line[4], (STRING_LENGTH, FOCUS_CHANNELS), jnp.float32, -0.7, 0.7)
    equality_indicator = jnp.any(jnp.arange(STRING_LENGTH)[:, None] == spike_location[None, :], axis=1)
    odds_correction = jnp.clip(base[None, :] + jnp.repeat(block_shift, TOK_DEV, axis=0) + jitter, -14.0, 0.0)
    odds_correction = jnp.where(equality_indicator[:, None] & lagging_fraction[None, :], -1.0 + 0.4 * spike_displacement_jitter, odds_correction)
    return odds_correction.astype(jnp.bfloat16)


def steps_of(stream_key, dims, shards, low, top_value):
    def one(position, blocks):
        draws = jax.random.uniform(jax.random.fold_in(jax.random.fold_in(stream_key, 6), position), (blocks,), jnp.float32, low / len(shards), top_value / len(shards))
        return jnp.repeat(jnp.exp(draws), dims[position] // blocks).reshape((-1,) + (1,) * (len(dims) - position - 1))

    level = one(*shards[0])
    for cut in shards[1:]:
        level = level * one(*cut)
    return level


def normal_values(rng, shape, deviation, limit, cuts=(), kind=jnp.bfloat16):
    drawn = jax.random.normal(rng, shape, jnp.float32) * deviation
    if len(cuts) > 0:
        drawn = steps_of(rng, shape, cuts, -0.22, 0.18) * drawn
    return jnp.clip(drawn, min=-limit, max=limit).astype(kind)


def setup_inputs(seed: int = 0) -> dict:
    key_of = jax.random.split(jax.random.key(seed), 13)
    return {
        "queries": normal_values(key_of[0], (STRING_LENGTH, FOCUS_CHANNELS * HEAD_DIM), 1.0, 6.0, ((0, 16), (1, 8))),
        "keys": normal_values(key_of[1], (STRING_LENGTH, FOCUS_CHANNELS * HEAD_DIM), 1.0, 6.0, ((0, 16), (1, 8))),
        "values": draw_values(jax.random.fold_in(key_of[12], 71), 0),
        "stick_bias": draw_stick_bias(jax.random.fold_in(key_of[12], 71), 0),
        "residual": normal_values(key_of[4], (STRING_LENGTH, D), 1.0, 6.0, ((0, 128),)),
        "out_weight": normal_values(key_of[5], (FOCUS_CHANNELS * HEAD_DIM, D), (FOCUS_CHANNELS * HEAD_DIM) ** -0.5, 0.1875),
        "norm_gain": jnp.clip(1.0 + 0.18 * jax.random.normal(key_of[6], (D,), jnp.float32), 0.1, 1.9),
        "gate_weight": normal_values(key_of[7], (D, FF), D ** -0.5, 0.125, ((0, 16), (1, 8))),
        "value_weight": normal_values(key_of[8], (D, FF), D ** -0.5, 0.125, ((0, 16), (1, 8))),
        "down_weight": normal_values(key_of[9], (D, FF), FF ** -0.5, 0.078125, ((0, 16), (1, 8))),
        "conv_gate": normal_values(key_of[10], (WIDTH, FF), WIDTH ** -0.5, 3.5, ((1, 8),), jnp.float32),
        "conv_value": normal_values(key_of[11], (WIDTH, FF), WIDTH ** -0.5, 3.5, ((1, 8),), jnp.float32),
    }


EPS = 1e-06

def round_keep(value):
    return lax.optimization_barrier(value.astype(jnp.bfloat16)).astype(jnp.float32)

def depthwise(upward, taps):
    extended = jnp.concatenate([jnp.zeros((2, upward.shape[1]), jnp.float32), upward.astype(jnp.float32)], axis=0)
    return taps[0] * extended[:-2] + taps[1] * extended[1:-1] + taps[2] * extended[2:]

def reference(queries, keys, values, stick_bias, residual, out_weight, norm_gain, gate_weight, value_weight, down_weight, conv_gate, conv_value):
    length = queries.shape[0]
    query_heads = queries.astype(jnp.float32).reshape(length, FOCUS_CHANNELS, HEAD_DIM).transpose(1, 0, 2)
    key_heads = keys.astype(jnp.float32).reshape(length, FOCUS_CHANNELS, HEAD_DIM).transpose(1, 0, 2)
    value_heads = values.astype(jnp.float32).reshape(length, FOCUS_CHANNELS, HEAD_DIM).transpose(1, 0, 2)
    bias_heads = stick_bias.astype(jnp.float32).T
    positions = jnp.arange(length, dtype=jnp.int32)
    blocks = length // TOK_DEV
    scale = HEAD_DIM ** (-0.5)

    def one_block(args):
        head, block = args
        query_block = lax.dynamic_slice_in_dim(query_heads[head], (block * TOK_DEV).astype(jnp.int32), TOK_DEV, 0)
        scores = jnp.dot(query_block, key_heads[head].T, preferred_element_type=jnp.float32) * scale + bias_heads[head][None, :]
        query_pos = block * TOK_DEV + jnp.arange(TOK_DEV, dtype=jnp.int32)
        before = positions[None, :] < query_pos[:, None]
        log_keep = jnp.where(before, jax.nn.log_sigmoid(-scores), 0.0)
        after = lax.cumsum(log_keep, axis=1, reverse=True) - log_keep
        stick = jnp.where(before, jnp.exp(jax.nn.log_sigmoid(scores) + after), 0.0)
        stick = round_keep(stick)
        return jnp.dot(stick, value_heads[head], preferred_element_type=jnp.float32)
    head_index = jnp.repeat(jnp.arange(FOCUS_CHANNELS, dtype=jnp.int32), blocks)
    block_index = jnp.tile(jnp.arange(blocks, dtype=jnp.int32), FOCUS_CHANNELS)
    outputs = lax.map(one_block, (head_index, block_index))
    attended = outputs.reshape(FOCUS_CHANNELS, length, HEAD_DIM).transpose(1, 0, 2).reshape(length, FOCUS_CHANNELS * HEAD_DIM).astype(jnp.bfloat16)
    group_cols = FOCUS_CHANNELS * HEAD_DIM // N_TP
    projected = jnp.zeros((length, D), jnp.float32)
    for group in range(N_TP):
        part = jnp.dot(attended[:, group * group_cols:(group + 1) * group_cols], out_weight[group * group_cols:(group + 1) * group_cols], preferred_element_type=jnp.float32)
        projected = projected + round_keep(part)
    middle = (residual.astype(jnp.float32) + projected).astype(jnp.bfloat16)
    middle_f = middle.astype(jnp.float32)
    normed = (middle_f * lax.rsqrt(lax.optimization_barrier(jnp.mean(middle_f * middle_f, axis=-1, keepdims=True)) + EPS) * norm_gain).astype(jnp.bfloat16)
    gate_up = jnp.dot(normed, gate_weight, preferred_element_type=jnp.float32).astype(jnp.bfloat16)
    value_up = jnp.dot(normed, value_weight, preferred_element_type=jnp.float32).astype(jnp.bfloat16)
    hidden = (jax.nn.silu(depthwise(gate_up, conv_gate)) * depthwise(value_up, conv_value)).astype(jnp.bfloat16)
    unit_cols = FF // N_TP
    down_total = jnp.zeros((length, D), jnp.float32)
    for group in range(N_TP):
        part = jnp.dot(hidden[:, group * unit_cols:(group + 1) * unit_cols], down_weight[:, group * unit_cols:(group + 1) * unit_cols].T, preferred_element_type=jnp.float32)
        down_total = down_total + round_keep(part)
    return (middle_f + down_total).astype(jnp.bfloat16)
```

```python
import jax
import jax.numpy as jnp
from jax import lax
from jax.experimental import pallas as pl
from jax.experimental.pallas import tpu as pltpu
from jax.sharding import PartitionSpec as P

EPS = 1e-06
LOG2E = 1.4426950408889634
NT = (((1,), (1,)), ((), ()))
CHUNK = 256
PAD = 16


def from_behind(block, axis, distance):
    devices = range(lax.axis_size(axis))
    route = [(i - distance, i) for i in devices if i - distance in devices]
    return lax.ppermute(block, axis, route)


def tri_matrix():
    rows = lax.broadcasted_iota(jnp.int32, (CHUNK, CHUNK), 0)
    cols = lax.broadcasted_iota(jnp.int32, (CHUNK, CHUNK), 1)
    return (rows > cols).astype(jnp.bfloat16), rows > cols


def visit_chunk(q, k, v, bias, tri, gone, acc, mask=None):
    scale = 128 ** (-0.5) * LOG2E
    s = lax.dot_general(q, k, NT, preferred_element_type=jnp.float32) * scale + bias
    if mask is not None:
        s = jnp.where(mask, s, -1e30)
    soft = jnp.maximum(jnp.log(1.0 + jnp.exp2(jnp.minimum(s, 126.0))) * LOG2E, s)
    behind = jnp.dot(soft.astype(jnp.bfloat16), tri, preferred_element_type=jnp.float32)
    stick = jnp.exp2((s - soft) - (behind + gone)).astype(jnp.bfloat16)
    acc = acc + jnp.dot(stick, v, preferred_element_type=jnp.float32)
    gone = gone + (behind[:, 0:1] + soft[:, 0:1])
    return gone, acc


def attention_kernel(q_ref, kv_ref, o_ref, acc_ref, gone_ref):
    rows, head = q_ref.shape
    stride = rows + PAD
    chunks = rows // CHUNK
    me = lax.axis_index("sp")
    tri, lower = tri_matrix()

    def load(block, c):
        at = pl.ds(pl.multiple_of(block * stride + c * CHUNK, 16), CHUNK)
        return kv_ref[at, :head], kv_ref[at, head:]

    def biases(block):
        at = pl.ds(pl.multiple_of(block * stride + rows, 16), PAD)
        return kv_ref[at, :].astype(jnp.float32) * LOG2E

    bias = biases(me)
    for t in range(chunks):
        here = slice(t * CHUNK, (t + 1) * CHUNK)
        q = q_ref[here, :]
        gone = jnp.zeros((CHUNK, 1), jnp.float32)
        acc = jnp.zeros((CHUNK, head), jnp.float32)
        for c in range(t, -1, -1):
            k, v = load(me, c)
            gone, acc = visit_chunk(
                q, k, v, bias[c : c + 1, :], tri, gone, acc, lower if c == t else None
            )
        acc_ref[here, :] = acc
        gone_ref[here, :] = jnp.broadcast_to(gone, (CHUNK, head))

    def block_step(step, carry):
        block = me - 1 - step
        gone, acc = carry
        bias = biases(block)
        for c in range(chunks - 1, -1, -1):
            k, v = load(block, c)
            gone, acc = visit_chunk(q_ref[...], k, v, bias[c : c + 1, :], tri, gone, acc)
        return gone, acc

    gone, acc = lax.fori_loop(0, me, block_step, (gone_ref[:, 0:1], acc_ref[...]))
    o_ref[...] = acc.astype(o_ref.dtype)


def attention(queries, kv_all):
    rows, head = queries.shape
    vmem = pl.BlockSpec(memory_space=pltpu.VMEM)
    return pl.pallas_call(
        attention_kernel,
        out_shape=jax.ShapeDtypeStruct((rows, head), jnp.bfloat16),
        in_specs=[vmem, vmem],
        out_specs=vmem,
        scratch_shapes=[
            pltpu.VMEM((rows, head), jnp.float32),
            pltpu.VMEM((rows, head), jnp.float32),
        ],
        compiler_params=pltpu.CompilerParams(vmem_limit_bytes=48 * 2**20),
        cost_estimate=pl.CostEstimate(
            flops=16 * 6 * rows * rows * head, bytes_accessed=9 * 2**20, transcendentals=0
        ),
        name="attention",
    )(queries, kv_all)


def local(
    queries,
    keys,
    values,
    stick_bias,
    residual,
    out_weight,
    norm_gain,
    gate_weight,
    value_weight,
    down_weight,
    conv_gate,
    conv_value,
):
    rows_here = queries.shape[0]
    model_width = residual.shape[1]
    bias_rows = stick_bias.reshape(rows_here // CHUNK, CHUNK)
    kv = jnp.concatenate(
        [
            jnp.concatenate([keys, values], axis=1),
            jnp.pad(bias_rows, ((0, PAD - bias_rows.shape[0]), (0, 0))),
        ],
        axis=0,
    )
    kv_all = lax.all_gather(kv, "sp", axis=0, tiled=True)
    whole_gate = lax.all_gather(gate_weight, "sp", axis=0, tiled=True)
    whole_value = lax.all_gather(value_weight, "sp", axis=0, tiled=True)
    whole_down = lax.all_gather(down_weight, "sp", axis=0, tiled=True)
    attended = attention(queries, kv_all)
    row_heads = lax.all_to_all(attended, "tp", split_axis=0, concat_axis=1, tiled=True)
    projected = jnp.dot(row_heads, out_weight, preferred_element_type=jnp.float32)
    middle_f = (residual.astype(jnp.float32) + projected).astype(jnp.bfloat16).astype(jnp.float32)
    normed = (
        middle_f
        * lax.rsqrt(jnp.mean(middle_f * middle_f, axis=-1, keepdims=True) + EPS)
        * norm_gain
    ).astype(jnp.bfloat16)
    piece = lax.all_gather(normed, "tp", axis=0, tiled=True)
    gate_up = jnp.dot(piece, whole_gate, preferred_element_type=jnp.float32).astype(jnp.bfloat16)
    value_up = jnp.dot(piece, whole_value, preferred_element_type=jnp.float32).astype(jnp.bfloat16)
    rim_gate, rim_value = from_behind((gate_up[-2:], value_up[-2:]), "sp", 1)

    def depthwise(rim, upward, taps):
        extended = jnp.concatenate([rim, upward], axis=0).astype(jnp.float32)
        return taps[0] * extended[:-2] + taps[1] * extended[1:-1] + taps[2] * extended[2:]

    hidden = (
        jax.nn.silu(depthwise(rim_gate, gate_up, conv_gate))
        * depthwise(rim_value, value_up, conv_value)
    ).astype(jnp.bfloat16)
    down = lax.dot_general(hidden, whole_down, NT, preferred_element_type=jnp.float32)
    down_total = lax.psum_scatter(
        down.astype(jnp.bfloat16), "tp", scatter_dimension=0, tiled=True
    ).astype(jnp.float32)
    return (middle_f + down_total).astype(jnp.bfloat16)


def solution(mesh):
    in_specs = (
        P("sp", "tp"),
        P("sp", "tp"),
        P("sp", "tp"),
        P("sp", "tp"),
        P(("sp", "tp"), None),
        P(),
        P(),
        P("sp", "tp"),
        P("sp", "tp"),
        P("sp", "tp"),
        P(None, "tp"),
        P(None, "tp"),
    )
    out_specs = P(("sp", "tp"), None)
    return jax.shard_map(local, mesh=mesh, in_specs=in_specs, out_specs=out_specs, check_vma=False)
```

```python
import jax
import jax.numpy as jnp
from jax import lax
from jax.experimental import pallas as pl
from jax.experimental.pallas import tpu as pltpu
from jax.sharding import PartitionSpec as P

EPS = 1e-06
LOG2E = 1.4426950408889634
NT = (((1,), (1,)), ((), ()))
CHUNK = 256
PAD = 16
SIDE = 4


def from_behind(block, axis, distance):
    devices = range(lax.axis_size(axis))
    route = [(i - distance, i) for i in devices if i - distance in devices]
    return lax.ppermute(block, axis, route)


def tri_matrix():
    rows = lax.broadcasted_iota(jnp.int32, (CHUNK, CHUNK), 0)
    cols = lax.broadcasted_iota(jnp.int32, (CHUNK, CHUNK), 1)
    return (rows > cols).astype(jnp.bfloat16), rows > cols


def visit_chunk(q, k, v, bias, tri, gone, acc, mask=None):
    scale = 128 ** (-0.5) * LOG2E
    s = lax.dot_general(q, k, NT, preferred_element_type=jnp.float32) * scale + bias
    if mask is not None:
        s = jnp.where(mask, s, -1e30)
    soft = jnp.maximum(jnp.log(1.0 + jnp.exp2(jnp.minimum(s, 126.0))) * LOG2E, s)
    behind = jnp.dot(soft.astype(jnp.bfloat16), tri, preferred_element_type=jnp.float32)
    stick = jnp.exp2((s - soft) - (behind + gone)).astype(jnp.bfloat16)
    acc = acc + jnp.dot(stick, v, preferred_element_type=jnp.float32)
    gone = gone + (behind[:, 0:1] + soft[:, 0:1])
    return gone, acc


def position():
    me = lax.axis_index("sp")
    return me, me // SIDE, me % SIDE


def exchange_kernel(q_ref, k_ref, v_ref, b_ref, qs_ref, ks_ref, vs_ref, bs_ref, send_sem, recv_sem, q_send, q_recv):
    me, z, y = position()
    quarter = q_ref.shape[0] // SIDE

    def copy_row(d, part):
        src, dst = ((k_ref, ks_ref), (v_ref, vs_ref), (b_ref, bs_ref))[part]
        return pltpu.make_async_remote_copy(
            src_ref=src,
            dst_ref=dst.at[y],
            send_sem=send_sem.at[part, d],
            recv_sem=recv_sem.at[part, y],
            device_id={"sp": z * SIDE + (y + d) % SIDE},
            device_id_type=pl.DeviceIdType.MESH,
        )

    def copy_query(dz, dy):
        to_y = (y + dy) % SIDE
        return pltpu.make_async_remote_copy(
            src_ref=q_ref.at[pl.ds(pl.multiple_of(to_y * quarter, quarter), quarter)],
            dst_ref=qs_ref.at[me],
            send_sem=q_send.at[dz, dy],
            recv_sem=q_recv.at[me],
            device_id={"sp": (z - dz) * SIDE + to_y},
            device_id_type=pl.DeviceIdType.MESH,
        )

    def for_queries(act):
        for dz in range(SIDE):
            for dy in range(SIDE):
                if dz or dy:

                    @pl.when(z >= dz)
                    def _():
                        act(copy_query(dz, dy))

    for d in (2, 1, 3):
        for part in range(3):
            copy_row(d, part).start()
    for_queries(lambda copy: copy.start())
    for d in (1, 3, 2):
        slot = (y + d) % SIDE
        for part in range(3):
            dst = (ks_ref, vs_ref, bs_ref)[part].at[slot]
            pltpu.make_async_copy(dst, dst, recv_sem.at[part, slot]).wait()
    for slot in range(SIDE * SIDE):

        @pl.when((slot // SIDE >= z) & (slot != me))
        def _():
            dst = qs_ref.at[slot]
            pltpu.make_async_copy(dst, dst, q_recv.at[slot]).wait()

    for d in (1, 2, 3):
        for part in range(3):
            copy_row(d, part).wait_send()
    for_queries(lambda copy: copy.wait_send())


def exchange(queries, keys, values, bias_rows):
    rows, head = queries.shape
    anywhere = pl.BlockSpec(memory_space=pl.ANY)
    count = SIDE * SIDE
    return pl.pallas_call(
        exchange_kernel,
        out_shape=(
            jax.ShapeDtypeStruct((count, rows // SIDE, head), jnp.bfloat16),
            jax.ShapeDtypeStruct((SIDE, rows, head), jnp.bfloat16),
            jax.ShapeDtypeStruct((SIDE, rows, head), jnp.bfloat16),
            jax.ShapeDtypeStruct((SIDE,) + bias_rows.shape, jnp.bfloat16),
        ),
        in_specs=[anywhere] * 4,
        out_specs=[anywhere] * 4,
        scratch_shapes=[
            pltpu.SemaphoreType.DMA((3, SIDE)),
            pltpu.SemaphoreType.DMA((3, SIDE)),
            pltpu.SemaphoreType.DMA((SIDE, SIDE)),
            pltpu.SemaphoreType.DMA((count,)),
        ],
        compiler_params=pltpu.CompilerParams(has_side_effects=True),
        cost_estimate=pl.CostEstimate(flops=10**10, bytes_accessed=4 * 2**20, transcendentals=0),
        name="exchange",
    )(queries, keys, values, bias_rows)


def attention_kernel(
    q_ref, k_ref, v_ref, b_ref, qs_ref, ks_ref, vs_ref, bs_ref,
    o_ref, g_ref, q_all, k_all, v_all, b_all, acc_ref, gone_ref, kv_sem, q_sem,
):
    rows, head = q_ref.shape
    quarter = rows // SIDE
    chunks = rows // CHUNK
    me, z, y = position()
    tri, _ = tri_matrix()
    own = (k_ref, v_ref, b_ref)
    others = (ks_ref, vs_ref, bs_ref)
    wholes = (k_all, v_all, b_all)

    for slot in range(SIDE - 1, -1, -1):
        for part in range(3):

            @pl.when(slot == y)
            def _():
                pltpu.make_async_copy(own[part], wholes[part].at[slot], kv_sem.at[part, slot]).start()

            @pl.when(slot != y)
            def _():
                pltpu.make_async_copy(
                    others[part].at[slot], wholes[part].at[slot], kv_sem.at[part, slot]
                ).start()

    for slot in range(SIDE * SIDE):
        dst = q_all.at[pl.ds(slot * quarter, quarter)]

        @pl.when(slot == me)
        def _():
            src = q_ref.at[pl.ds(pl.multiple_of(y * quarter, quarter), quarter)]
            pltpu.make_async_copy(src, dst, q_sem.at[slot]).start()

        @pl.when((slot // SIDE >= z) & (slot != me))
        def _():
            pltpu.make_async_copy(qs_ref.at[slot], dst, q_sem.at[slot]).start()

    for slot in range(SIDE * SIDE):

        @pl.when(slot // SIDE >= z)
        def _():
            dst = q_all.at[pl.ds(slot * quarter, quarter)]
            pltpu.make_async_copy(qs_ref.at[slot], dst, q_sem.at[slot]).wait()

    for slot in range(SIDE):
        for part in range(3):
            pltpu.make_async_copy(
                others[part].at[slot], wholes[part].at[slot], kv_sem.at[part, slot]
            ).wait()

    def finish(group, gone, acc):
        for m in range(SIDE):
            here = slice(m * quarter, (m + 1) * quarter)
            o_ref[group * SIDE + m] = acc[here].astype(o_ref.dtype)
            turned = jnp.broadcast_to(gone[here], (quarter, 128)).T
            for half in range(2):
                g_ref[group * SIDE + m, half] = turned[0:8, half * 128 : (half + 1) * 128]

    acc_ref[...] = jnp.zeros_like(acc_ref)
    gone_ref[...] = jnp.zeros_like(gone_ref)
    for j in range(SIDE - 1, -1, -1):
        low = j * quarter
        size = rows - low
        q = q_all[pl.ds(pl.multiple_of(z * rows + low, quarter), size), :]
        bias = b_all[j].astype(jnp.float32) * LOG2E
        acc = acc_ref[low:, :]
        gone = gone_ref[low:, 0:1]
        row = lax.broadcasted_iota(jnp.int32, (size, CHUNK), 0)
        col = lax.broadcasted_iota(jnp.int32, (size, CHUNK), 1)
        for c in range(chunks - 1, -1, -1):
            at = slice(c * CHUNK, (c + 1) * CHUNK)
            mask = (row >= quarter) | (col - row < y * quarter - c * CHUNK)
            gone, acc = visit_chunk(
                q, k_all[j, at, :], v_all[j, at, :], bias[c : c + 1, :], tri, gone, acc, mask
            )
        acc_ref[low:, :] = acc
        gone_ref[low:, :] = jnp.broadcast_to(gone, (size, 128))
    finish(z, gone_ref[:, 0:1], acc_ref[...])

    def group_step(group, carry):
        q = q_all[pl.ds(pl.multiple_of(group * rows, rows), rows), :]

        def block_step(step, state):
            gone, acc = state
            j = SIDE - 1 - step
            bias = b_all[j].astype(jnp.float32) * LOG2E
            for c in range(chunks - 1, -1, -1):
                at = slice(c * CHUNK, (c + 1) * CHUNK)
                gone, acc = visit_chunk(
                    q, k_all[j, at, :], v_all[j, at, :], bias[c : c + 1, :], tri, gone, acc
                )
            return gone, acc

        start = (jnp.zeros((rows, 1), jnp.float32), jnp.zeros((rows, head), jnp.float32))
        gone, acc = lax.fori_loop(0, SIDE, block_step, start)
        finish(group, gone, acc)
        return carry

    lax.fori_loop(z + 1, SIDE, group_step, 0)


def attention(queries, keys, values, bias_rows, q_parts, k_parts, v_parts, b_parts):
    rows, head = queries.shape
    anywhere = pl.BlockSpec(memory_space=pl.ANY)
    vmem = pl.BlockSpec(memory_space=pltpu.VMEM)
    count = SIDE * SIDE
    return pl.pallas_call(
        attention_kernel,
        out_shape=(
            jax.ShapeDtypeStruct((count, rows // SIDE, head), jnp.bfloat16),
            jax.ShapeDtypeStruct((count, 2, 8, 128), jnp.float32),
        ),
        in_specs=[anywhere] * 8,
        out_specs=[vmem, vmem],
        scratch_shapes=[
            pltpu.VMEM((SIDE * rows, head), jnp.bfloat16),
            pltpu.VMEM((SIDE, rows, head), jnp.bfloat16),
            pltpu.VMEM((SIDE, rows, head), jnp.bfloat16),
            pltpu.VMEM((SIDE,) + bias_rows.shape, jnp.bfloat16),
            pltpu.VMEM((rows, head), jnp.float32),
            pltpu.VMEM((rows, 128), jnp.float32),
            pltpu.SemaphoreType.DMA((3, SIDE)),
            pltpu.SemaphoreType.DMA((count,)),
        ],
        compiler_params=pltpu.CompilerParams(vmem_limit_bytes=48 * 2**20),
        cost_estimate=pl.CostEstimate(
            flops=14 * 6 * rows * rows * head, bytes_accessed=4 * 2**20, transcendentals=0
        ),
        name="attention",
    )(queries, keys, values, bias_rows, q_parts, k_parts, v_parts, b_parts)


def deliver_kernel(o_ref, g_ref, os_ref, gs_ref, send_sem, recv_sem):
    me, z, y = position()
    head = lax.axis_index("tp")
    owner_rows = os_ref.shape[2]

    def pieces(block, half):
        src = o_ref.at[block, pl.ds(half * owner_rows, owner_rows)]
        return ((src, os_ref), (g_ref.at[block, half], gs_ref))

    def remote(block, half, part):
        src, dst = pieces(block, half)[part]
        return pltpu.make_async_remote_copy(
            src_ref=src,
            dst_ref=dst.at[head, z],
            send_sem=send_sem.at[part, block, half],
            recv_sem=recv_sem.at[part, head, z],
            device_id={"sp": block, "tp": 2 * y + half},
            device_id_type=pl.DeviceIdType.MESH,
        )

    def local_copy(block, half, part):
        src, dst = pieces(block, half)[part]
        return pltpu.make_async_copy(src, dst.at[head, z], recv_sem.at[part, head, z])

    def is_me(block, half):
        return (block == me) & (2 * y + half == head)

    def send(block, carry):
        for half in range(2):

            @pl.when(is_me(block, half))
            def _():
                for part in range(2):
                    local_copy(block, half, part).start()

            @pl.when(jnp.logical_not(is_me(block, half)))
            def _():
                for part in range(2):
                    remote(block, half, part).start()

        return carry

    lax.fori_loop(z * SIDE, SIDE * SIDE, send, 0)

    def take(group, carry):
        for h in range(os_ref.shape[0]):
            for part in range(2):
                dst = (os_ref, gs_ref)[part].at[h, group]
                pltpu.make_async_copy(dst, dst, recv_sem.at[part, h, group]).wait()
        return carry

    lax.fori_loop(0, z + 1, take, 0)

    def sent(block, carry):
        for half in range(2):

            @pl.when(jnp.logical_not(is_me(block, half)))
            def _():
                for part in range(2):
                    remote(block, half, part).wait_send()

        return carry

    lax.fori_loop(z * SIDE, SIDE * SIDE, sent, 0)


def deliver(outs, logs, heads):
    count, quarter, head = outs.shape
    vmem = pl.BlockSpec(memory_space=pltpu.VMEM)
    return pl.pallas_call(
        deliver_kernel,
        out_shape=(
            jax.ShapeDtypeStruct((heads, SIDE, quarter // 2, head), jnp.bfloat16),
            jax.ShapeDtypeStruct((heads, SIDE, 8, 128), jnp.float32),
        ),
        in_specs=[vmem, vmem],
        out_specs=[vmem, vmem],
        scratch_shapes=[
            pltpu.SemaphoreType.DMA((2, count, 2)),
            pltpu.SemaphoreType.DMA((2, heads, SIDE)),
        ],
        compiler_params=pltpu.CompilerParams(has_side_effects=True),
        cost_estimate=pl.CostEstimate(flops=5 * 10**9, bytes_accessed=4 * 2**20, transcendentals=0),
        name="deliver",
    )(outs, logs)


def combine(parts, logs):
    group = lax.axis_index("sp") // SIDE
    valid = jnp.arange(SIDE) <= group
    left = jnp.where(valid[None, :, None], logs[:, :, 0, :], 0.0)
    later = jnp.flip(jnp.cumsum(jnp.flip(left, 1), axis=1), 1) - left
    weight = jnp.where(valid[None, :, None], jnp.exp2(-later), 0.0)
    terms = jnp.where(valid[None, :, None, None], parts.astype(jnp.float32), 0.0)
    total = jnp.sum(terms * weight[..., None], axis=1)
    return total.transpose(1, 0, 2).reshape(total.shape[1], -1).astype(jnp.bfloat16)


def local(
    queries,
    keys,
    values,
    stick_bias,
    residual,
    out_weight,
    norm_gain,
    gate_weight,
    value_weight,
    down_weight,
    conv_gate,
    conv_value,
):
    rows_here = queries.shape[0]
    model_width = residual.shape[1]
    bias_rows = stick_bias.reshape(rows_here // CHUNK, CHUNK)
    bias_rows = jnp.pad(bias_rows, ((0, PAD - bias_rows.shape[0]), (0, 0)))
    units = gate_weight.shape[1]
    shared = exchange(queries, keys, values, bias_rows)
    weights = jnp.concatenate([gate_weight, value_weight, down_weight], axis=1)
    weights, shared = lax.optimization_barrier((weights, shared))
    whole = lax.all_gather(weights, "sp", axis=0, tiled=True)
    whole_gate, whole_value, whole_down = (whole[:, k * units : (k + 1) * units] for k in range(3))
    outs, logs = attention(queries, keys, values, bias_rows, *shared)
    row_heads = combine(*deliver(outs, logs, lax.axis_size("tp")))
    projected = jnp.dot(row_heads, out_weight, preferred_element_type=jnp.float32)
    middle_f = (residual.astype(jnp.float32) + projected).astype(jnp.bfloat16).astype(jnp.float32)
    normed = (
        middle_f
        * lax.rsqrt(jnp.mean(middle_f * middle_f, axis=-1, keepdims=True) + EPS)
        * norm_gain
    ).astype(jnp.bfloat16)
    piece = lax.all_gather(normed, "tp", axis=0, tiled=True)
    gate_up = jnp.dot(piece, whole_gate, preferred_element_type=jnp.float32).astype(jnp.bfloat16)
    value_up = jnp.dot(piece, whole_value, preferred_element_type=jnp.float32).astype(jnp.bfloat16)
    rim_gate, rim_value = from_behind((gate_up[-2:], value_up[-2:]), "sp", 1)

    def depthwise(rim, upward, taps):
        extended = jnp.concatenate([rim, upward], axis=0).astype(jnp.float32)
        return taps[0] * extended[:-2] + taps[1] * extended[1:-1] + taps[2] * extended[2:]

    hidden = (
        jax.nn.silu(depthwise(rim_gate, gate_up, conv_gate))
        * depthwise(rim_value, value_up, conv_value)
    ).astype(jnp.bfloat16)
    down = lax.dot_general(hidden, whole_down, NT, preferred_element_type=jnp.float32)
    down_total = lax.psum_scatter(
        down.astype(jnp.bfloat16), "tp", scatter_dimension=0, tiled=True
    ).astype(jnp.float32)
    return (middle_f + down_total).astype(jnp.bfloat16)


def solution(mesh):
    in_specs = (
        P("sp", "tp"),
        P("sp", "tp"),
        P("sp", "tp"),
        P("sp", "tp"),
        P(("sp", "tp"), None),
        P(),
        P(),
        P("sp", "tp"),
        P("sp", "tp"),
        P("sp", "tp"),
        P(None, "tp"),
        P(None, "tp"),
    )
    out_specs = P(("sp", "tp"), None)
    return jax.shard_map(local, mesh=mesh, in_specs=in_specs, out_specs=out_specs, check_vma=False)
```

```python
import jax
import jax.numpy as jnp
from jax import lax
from jax.experimental import pallas as pl
from jax.experimental.pallas import tpu as pltpu
from jax.sharding import PartitionSpec as P

EPS = 1e-06
LOG2E = 1.4426950408889634
NT = (((1,), (1,)), ((), ()))
CHUNK = 256
PAD = 16
SIDE = 4
RIM = 16


def tri_matrix():
    rows = lax.broadcasted_iota(jnp.int32, (CHUNK, CHUNK), 0)
    cols = lax.broadcasted_iota(jnp.int32, (CHUNK, CHUNK), 1)
    return (rows > cols).astype(jnp.bfloat16), rows > cols


def visit_chunk(q, k, v, bias, tri, gone, acc, mask=None):
    scale = 128 ** (-0.5) * LOG2E
    s = lax.dot_general(q, k, NT, preferred_element_type=jnp.float32) * scale + bias
    if mask is not None:
        s = jnp.where(mask, s, -1e30)
    soft = jnp.maximum(jnp.log(1.0 + jnp.exp2(jnp.minimum(s, 126.0))) * LOG2E, s)
    behind = jnp.dot(soft.astype(jnp.bfloat16), tri, preferred_element_type=jnp.float32)
    stick = jnp.exp2((s - soft) - (behind + gone)).astype(jnp.bfloat16)
    acc = acc + jnp.dot(stick, v, preferred_element_type=jnp.float32)
    gone = gone + (behind[:, 0:1] + soft[:, 0:1])
    return gone, acc


def position():
    me = lax.axis_index("sp")
    return me, me // SIDE, me % SIDE


def owners_of(y):
    core = lax.axis_index("tp") % 2
    return 2 * ((y + core) % SIDE), 2 * ((y + core + 2) % SIDE) + 1


def remote_copy(src, dst, send_sem, recv_sem, **where):
    return pltpu.make_async_remote_copy(
        src_ref=src,
        dst_ref=dst,
        send_sem=send_sem,
        recv_sem=recv_sem,
        device_id=where,
        device_id_type=pl.DeviceIdType.MESH,
    )


def arrived(dst, sem):
    pltpu.make_async_copy(dst, dst, sem).wait()


def exchange_kernel(
    q_ref, k_ref, v_ref, b_ref, qs_ref, ks_ref, vs_ref, bs_ref,
    send_sem, recv_sem, bias_send, bias_recv, q_send, q_recv, own_sem, z_send, z_recv,
):
    me, z, y = position()
    share = q_ref.shape[0] // (2 * SIDE)
    right = (y + 1) % SIDE
    left = (y + 3) % SIDE
    across = (y + 2) % SIDE
    row = z * SIDE

    def hop(part, src_slot, to, lane):
        src = (k_ref, v_ref)[part] if src_slot is None else (ks_ref, vs_ref)[part].at[src_slot]
        slot = y if src_slot is None else src_slot
        return remote_copy(
            src,
            (ks_ref, vs_ref)[part].at[slot],
            send_sem.at[part, lane],
            recv_sem.at[part, slot],
            sp=row + to,
        )

    def bias_hop(d):
        return remote_copy(
            b_ref, bs_ref.at[y], bias_send.at[d], bias_recv.at[y], sp=row + (y + d) % SIDE
        )

    def q_piece(of, half, act_remote, d):
        src = q_ref.at[pl.ds(pl.multiple_of(owners_of(of)[half] * share, share), share)]
        dst = qs_ref.at[me, pl.ds(half * share, share)]
        if act_remote:
            return remote_copy(
                src, dst, q_send.at[d, half], q_recv.at[me % SIDE, half], sp=row + of
            )
        return pltpu.make_async_copy(src, dst, own_sem.at[half])

    for half in range(2):
        q_piece(y, half, False, 0).start()
    for d in (2, 1, 3):
        for half in range(2):
            q_piece((y + d) % SIDE, half, True, d).start()
        bias_hop(d).start()
    hop(0, None, right, 0).start()
    hop(1, None, left, 0).start()
    hop(1, None, right, 1).start()
    hop(0, None, left, 1).start()

    for half in range(2):
        q_piece(y, half, False, 0).wait()
        for d in (1, 2, 3):
            slot = (y + d) % SIDE
            arrived(qs_ref.at[row + slot, pl.ds(half * share, share)], q_recv.at[slot, half])

    def down_row(dz):
        ours = qs_ref.at[pl.ds(pl.multiple_of(row, SIDE), SIDE)]
        return remote_copy(ours, ours, z_send.at[dz], z_recv.at[z], sp=row - dz * SIDE + y)

    for dz in (2, 3, 1):

        @pl.when(z >= dz)
        def _():
            down_row(dz).start()

    arrived(ks_ref.at[left], recv_sem.at[0, left])
    hop(0, left, right, 2).start()
    arrived(vs_ref.at[right], recv_sem.at[1, right])
    hop(1, right, left, 2).start()
    arrived(vs_ref.at[left], recv_sem.at[1, left])
    arrived(ks_ref.at[right], recv_sem.at[0, right])
    arrived(ks_ref.at[across], recv_sem.at[0, across])
    arrived(vs_ref.at[across], recv_sem.at[1, across])
    for d in (1, 2, 3):
        slot = (y + d) % SIDE
        arrived(bs_ref.at[slot], bias_recv.at[slot])
    for other in range(1, SIDE):

        @pl.when(z < other)
        def _():
            arrived(qs_ref.at[pl.ds(other * SIDE, SIDE)], z_recv.at[other])

    hop(0, None, right, 0).wait_send()
    hop(1, None, left, 0).wait_send()
    hop(1, None, right, 1).wait_send()
    hop(0, None, left, 1).wait_send()
    hop(0, left, right, 2).wait_send()
    hop(1, right, left, 2).wait_send()
    for d in (1, 2, 3):
        bias_hop(d).wait_send()
        for half in range(2):
            q_piece((y + d) % SIDE, half, True, d).wait_send()
    for dz in (1, 2, 3):

        @pl.when(z >= dz)
        def _():
            down_row(dz).wait_send()


def exchange(queries, keys, values, bias_rows):
    rows, head = queries.shape
    anywhere = pl.BlockSpec(memory_space=pl.ANY)
    count = SIDE * SIDE
    dma = pltpu.SemaphoreType.DMA
    return pl.pallas_call(
        exchange_kernel,
        out_shape=(
            jax.ShapeDtypeStruct((count, rows // SIDE, head), jnp.bfloat16),
            jax.ShapeDtypeStruct((SIDE, rows, head), jnp.bfloat16),
            jax.ShapeDtypeStruct((SIDE, rows, head), jnp.bfloat16),
            jax.ShapeDtypeStruct((SIDE,) + bias_rows.shape, jnp.bfloat16),
        ),
        in_specs=[anywhere] * 4,
        out_specs=[anywhere] * 4,
        scratch_shapes=[
            dma((2, 3)), dma((2, SIDE)), dma((SIDE,)), dma((SIDE,)), dma((SIDE, 2)),
            dma((SIDE, 2)), dma((2,)), dma((SIDE,)), dma((SIDE,)),
        ],
        compiler_params=pltpu.CompilerParams(has_side_effects=True),
        cost_estimate=pl.CostEstimate(flops=10**10, bytes_accessed=4 * 2**20, transcendentals=0),
        name="exchange",
    )(queries, keys, values, bias_rows)


def attention_kernel(
    k_ref, v_ref, b_ref, qs_ref, ks_ref, vs_ref, bs_ref,
    o_ref, g_ref, q_all, k_all, v_all, b_all, acc_ref, gone_ref, kv_sem, q_sem,
):
    rows, head = k_ref.shape
    quarter = rows // SIDE
    chunks = rows // CHUNK
    _, z, y = position()
    first, second = (owner * (quarter // 2) for owner in owners_of(y))
    tri, _ = tri_matrix()
    own = (k_ref, v_ref, b_ref)
    others = (ks_ref, vs_ref, bs_ref)
    wholes = (k_all, v_all, b_all)

    for slot in range(SIDE - 1, -1, -1):
        for part in range(3):

            @pl.when(slot == y)
            def _():
                pltpu.make_async_copy(own[part], wholes[part].at[slot], kv_sem.at[part, slot]).start()

            @pl.when(slot != y)
            def _():
                pltpu.make_async_copy(
                    others[part].at[slot], wholes[part].at[slot], kv_sem.at[part, slot]
                ).start()

    for slot in range(SIDE * SIDE):
        dst = q_all.at[pl.ds(slot * quarter, quarter)]

        @pl.when(slot // SIDE >= z)
        def _():
            pltpu.make_async_copy(qs_ref.at[slot], dst, q_sem.at[slot]).start()

    for slot in range(SIDE * SIDE):

        @pl.when(slot // SIDE >= z)
        def _():
            dst = q_all.at[pl.ds(slot * quarter, quarter)]
            pltpu.make_async_copy(qs_ref.at[slot], dst, q_sem.at[slot]).wait()

    for slot in range(SIDE):
        for part in range(3):
            pltpu.make_async_copy(
                others[part].at[slot], wholes[part].at[slot], kv_sem.at[part, slot]
            ).wait()

    def finish(group, gone, acc):
        for m in range(SIDE):
            here = slice(m * quarter, (m + 1) * quarter)
            o_ref[group * SIDE + m] = acc[here].astype(o_ref.dtype)
            turned = jnp.broadcast_to(gone[here], (quarter, 128)).T
            for half in range(2):
                g_ref[group * SIDE + m, half] = turned[0:8, half * 128 : (half + 1) * 128]

    acc_ref[...] = jnp.zeros_like(acc_ref)
    gone_ref[...] = jnp.zeros_like(gone_ref)
    for j in range(SIDE - 1, -1, -1):
        low = j * quarter
        size = rows - low
        q = q_all[pl.ds(pl.multiple_of(z * rows + low, quarter), size), :]
        bias = b_all[j].astype(jnp.float32) * LOG2E
        acc = acc_ref[low:, :]
        gone = gone_ref[low:, 0:1]
        row = lax.broadcasted_iota(jnp.int32, (size, CHUNK), 0)
        col = lax.broadcasted_iota(jnp.int32, (size, CHUNK), 1)
        place = row + jnp.where(row < quarter // 2, first, second - quarter // 2)
        for c in range(chunks - 1, -1, -1):
            at = slice(c * CHUNK, (c + 1) * CHUNK)
            mask = (row >= quarter) | (col + c * CHUNK < place)
            gone, acc = visit_chunk(
                q, k_all[j, at, :], v_all[j, at, :], bias[c : c + 1, :], tri, gone, acc, mask
            )
        acc_ref[low:, :] = acc
        gone_ref[low:, :] = jnp.broadcast_to(gone, (size, 128))
    finish(z, gone_ref[:, 0:1], acc_ref[...])

    def group_step(group, carry):
        q = q_all[pl.ds(pl.multiple_of(group * rows, rows), rows), :]

        def block_step(step, state):
            gone, acc = state
            j = SIDE - 1 - step
            bias = b_all[j].astype(jnp.float32) * LOG2E
            for c in range(chunks - 1, -1, -1):
                at = slice(c * CHUNK, (c + 1) * CHUNK)
                gone, acc = visit_chunk(
                    q, k_all[j, at, :], v_all[j, at, :], bias[c : c + 1, :], tri, gone, acc
                )
            return gone, acc

        start = (jnp.zeros((rows, 1), jnp.float32), jnp.zeros((rows, head), jnp.float32))
        gone, acc = lax.fori_loop(0, SIDE, block_step, start)
        finish(group, gone, acc)
        return carry

    lax.fori_loop(z + 1, SIDE, group_step, 0)


def attention(keys, values, bias_rows, q_parts, k_parts, v_parts, b_parts):
    rows, head = keys.shape
    anywhere = pl.BlockSpec(memory_space=pl.ANY)
    vmem = pl.BlockSpec(memory_space=pltpu.VMEM)
    count = SIDE * SIDE
    return pl.pallas_call(
        attention_kernel,
        out_shape=(
            jax.ShapeDtypeStruct((count, rows // SIDE, head), jnp.bfloat16),
            jax.ShapeDtypeStruct((count, 2, 8, 128), jnp.float32),
        ),
        in_specs=[anywhere] * 7,
        out_specs=[vmem, vmem],
        scratch_shapes=[
            pltpu.VMEM((SIDE * rows, head), jnp.bfloat16),
            pltpu.VMEM((SIDE, rows, head), jnp.bfloat16),
            pltpu.VMEM((SIDE, rows, head), jnp.bfloat16),
            pltpu.VMEM((SIDE,) + bias_rows.shape, jnp.bfloat16),
            pltpu.VMEM((rows, head), jnp.float32),
            pltpu.VMEM((rows, 128), jnp.float32),
            pltpu.SemaphoreType.DMA((3, SIDE)),
            pltpu.SemaphoreType.DMA((count,)),
        ],
        compiler_params=pltpu.CompilerParams(vmem_limit_bytes=48 * 2**20),
        cost_estimate=pl.CostEstimate(
            flops=14 * 6 * rows * rows * head, bytes_accessed=4 * 2**20, transcendentals=0
        ),
        name="attention",
    )(keys, values, bias_rows, q_parts, k_parts, v_parts, b_parts)


def deliver_kernel(o_ref, g_ref, os_ref, gs_ref, send_sem, recv_sem):
    me, z, y = position()
    head = lax.axis_index("tp")
    owner_rows = os_ref.shape[2]
    owners = owners_of(y)

    def pieces(block, half):
        src = o_ref.at[block, pl.ds(half * owner_rows, owner_rows)]
        return ((src, os_ref), (g_ref.at[block, half], gs_ref))

    def remote(block, half, part):
        src, dst = pieces(block, half)[part]
        return pltpu.make_async_remote_copy(
            src_ref=src,
            dst_ref=dst.at[head, z],
            send_sem=send_sem.at[part, block, half],
            recv_sem=recv_sem.at[part, head, z],
            device_id={"sp": block, "tp": owners[half]},
            device_id_type=pl.DeviceIdType.MESH,
        )

    def local_copy(block, half, part):
        src, dst = pieces(block, half)[part]
        return pltpu.make_async_copy(src, dst.at[head, z], recv_sem.at[part, head, z])

    def is_me(block, half):
        return (block == me) & (owners[half] == head)

    def send(block, carry):
        for half in range(2):

            @pl.when(is_me(block, half))
            def _():
                for part in range(2):
                    local_copy(block, half, part).start()

            @pl.when(jnp.logical_not(is_me(block, half)))
            def _():
                for part in range(2):
                    remote(block, half, part).start()

        return carry

    lax.fori_loop(z * SIDE, SIDE * SIDE, send, 0)

    def take(group, carry):
        for h in range(os_ref.shape[0]):
            for part in range(2):
                dst = (os_ref, gs_ref)[part].at[h, group]
                pltpu.make_async_copy(dst, dst, recv_sem.at[part, h, group]).wait()
        return carry

    lax.fori_loop(0, z + 1, take, 0)

    def sent(block, carry):
        for half in range(2):

            @pl.when(jnp.logical_not(is_me(block, half)))
            def _():
                for part in range(2):
                    remote(block, half, part).wait_send()

        return carry

    lax.fori_loop(z * SIDE, SIDE * SIDE, sent, 0)


def deliver(outs, logs, heads):
    count, quarter, head = outs.shape
    vmem = pl.BlockSpec(memory_space=pltpu.VMEM)
    return pl.pallas_call(
        deliver_kernel,
        out_shape=(
            jax.ShapeDtypeStruct((heads, SIDE, quarter // 2, head), jnp.bfloat16),
            jax.ShapeDtypeStruct((heads, SIDE, 8, 128), jnp.float32),
        ),
        in_specs=[vmem, vmem],
        out_specs=[vmem, vmem],
        scratch_shapes=[
            pltpu.SemaphoreType.DMA((2, count, 2)),
            pltpu.SemaphoreType.DMA((2, heads, SIDE)),
        ],
        compiler_params=pltpu.CompilerParams(has_side_effects=True),
        cost_estimate=pl.CostEstimate(flops=5 * 10**9, bytes_accessed=4 * 2**20, transcendentals=0),
        name="deliver",
    )(outs, logs)


def combine(parts, logs):
    group = lax.axis_index("sp") // SIDE
    valid = jnp.arange(SIDE) <= group
    left = jnp.where(valid[None, :, None], logs[:, :, 0, :], 0.0)
    later = jnp.flip(jnp.cumsum(jnp.flip(left, 1), axis=1), 1) - left
    weight = jnp.where(valid[None, :, None], jnp.exp2(-later), 0.0)
    terms = jnp.where(valid[None, :, None, None], parts.astype(jnp.float32), 0.0)
    total = jnp.sum(terms * weight[..., None], axis=1)
    return total.transpose(1, 0, 2).reshape(total.shape[1], -1).astype(jnp.bfloat16)


def place_of():
    me = lax.axis_index("tp")
    return me // 2, me % 2


def gather_kernel(n_ref, all_ref, rim_ref, ring_send, ring_recv, twin_send, twin_recv, rim_send, rim_recv, own_sem):
    x, core = place_of()
    block = lax.axis_index("sp")
    rows = n_ref.shape[0]
    part = rows // 2
    right = (x + 1) % SIDE
    left = (x + 3) % SIDE
    across = (x + 2) % SIDE

    def spot(chip, half, of_core=None):
        of_core = core if of_core is None else of_core
        return all_ref.at[2 * chip + of_core, pl.ds(half * part, part)]

    def ring(chip, half, to, lane):
        src = n_ref.at[pl.ds(half * part, part)] if chip is None else spot(chip, half)
        chip = x if chip is None else chip
        return remote_copy(
            src, spot(chip, half), ring_send.at[lane, half], ring_recv.at[chip, half], tp=2 * to + core
        )

    def twin(chip, half):
        src = n_ref.at[pl.ds(half * part, part)] if chip is None else spot(chip, half)
        chip = x if chip is None else chip
        return remote_copy(
            src, spot(chip, half), twin_send.at[chip, half], twin_recv.at[chip, half], tp=2 * x + 1 - core
        )

    def rim(to):
        return remote_copy(
            n_ref.at[pl.ds(rows - RIM, RIM)], rim_ref, rim_send.at[to], rim_recv, sp=block + 1, tp=to
        )

    last = (x == SIDE - 1) & (core == 1) & (block < SIDE * SIDE - 1)
    own = pltpu.make_async_copy(n_ref, all_ref.at[2 * x + core], own_sem)
    ring(None, 0, right, 0).start()
    ring(None, 1, left, 1).start()
    ring(None, 1, right, 0).start()
    ring(None, 0, left, 1).start()
    own.start()
    for half in range(2):
        twin(None, half).start()

    @pl.when(last)
    def _():
        for to in range(2 * SIDE):
            rim(to).start()

    arrived(spot(left, 0), ring_recv.at[left, 0])
    ring(left, 0, right, 2).start()
    twin(left, 0).start()
    arrived(spot(right, 1), ring_recv.at[right, 1])
    ring(right, 1, left, 2).start()
    twin(right, 1).start()
    for chip, half in ((left, 1), (right, 0), (across, 0), (across, 1)):
        arrived(spot(chip, half), ring_recv.at[chip, half])
        twin(chip, half).start()
    own.wait()
    for chip in range(SIDE):
        for half in range(2):
            arrived(spot(chip, half, 1 - core), twin_recv.at[chip, half])

    @pl.when(block > 0)
    def _():
        arrived(rim_ref, rim_recv)

    for half in range(2):
        ring(None, half, right, 0).wait_send()
        ring(None, half, left, 1).wait_send()
        twin(None, half).wait_send()
        for chip in (left, right, across):
            twin(chip, half).wait_send()
    ring(left, 0, right, 2).wait_send()
    ring(right, 1, left, 2).wait_send()

    @pl.when(last)
    def _():
        for to in range(2 * SIDE):
            rim(to).wait_send()


def gather_rows(normed):
    rows, width = normed.shape
    vmem = pl.BlockSpec(memory_space=pltpu.VMEM)
    dma = pltpu.SemaphoreType.DMA
    return pl.pallas_call(
        gather_kernel,
        out_shape=(
            jax.ShapeDtypeStruct((2 * SIDE, rows, width), jnp.bfloat16),
            jax.ShapeDtypeStruct((RIM, width), jnp.bfloat16),
        ),
        in_specs=[vmem],
        out_specs=[vmem, vmem],
        scratch_shapes=[
            dma((3, 2)), dma((SIDE, 2)), dma((SIDE, 2)), dma((SIDE, 2)), dma((2 * SIDE,)), dma(()), dma(()),
        ],
        compiler_params=pltpu.CompilerParams(has_side_effects=True, vmem_limit_bytes=24 * 2**20),
        cost_estimate=pl.CostEstimate(flops=5 * 10**9, bytes_accessed=4 * 2**20, transcendentals=0),
        name="gather_rows",
    )(normed)


def feed_forward_kernel(
    x_ref, rim_ref, w_ref, cg_ref, cv_ref, out_ref, up_ref, down_ref, gate_ref, value_ref, w_sem
):
    blocks, rows, depth = x_ref.shape
    units = down_ref.shape[0]
    shards = w_ref.shape[0]
    deep = depth // shards
    tile = 2 * rows
    first = lax.axis_index("sp") == 0

    def weight_copies(k):
        at = slice(k * deep, (k + 1) * deep)
        return (
            pltpu.make_async_copy(
                w_ref.at[k, pl.ds(0, 2 * units)], up_ref.at[:, at], w_sem.at[0, k]
            ),
            pltpu.make_async_copy(
                w_ref.at[k, pl.ds(2 * units, units)], down_ref.at[:, at], w_sem.at[1, k]
            ),
        )

    for k in range(shards):
        for copy in weight_copies(k):
            copy.start()
    for k in range(shards):
        weight_copies(k)[0].wait()

    def up(x, which):
        w = up_ref[which * units : (which + 1) * units, :]
        return lax.dot_general(x, w, NT, preferred_element_type=jnp.float32)

    for which, ref in enumerate((gate_ref, value_ref)):
        rim = up(rim_ref[...], which)
        ref[0:RIM, :] = jnp.where(first, 0.0, rim)

    def conv(ref, taps, start):
        at = pl.multiple_of(start, tile)
        window = ref[pl.ds(at, tile + RIM), :]
        return (
            taps[0:1, :] * window[RIM - 2 : RIM - 2 + tile]
            + taps[1:2, :] * window[RIM - 1 : RIM - 1 + tile]
            + taps[2:3, :] * window[RIM : RIM + tile]
        )

    for k in range(shards):
        weight_copies(k)[1].wait()

    @pl.loop(0, blocks // 2)
    def _(t):
        x = x_ref[pl.ds(t * 2, 2)].reshape(tile, depth)
        start = t * tile
        for which, ref in enumerate((gate_ref, value_ref)):
            ref[pl.ds(pl.multiple_of(start + RIM, RIM), tile), :] = up(x, which)
        gate = conv(gate_ref, cg_ref, start)
        value = conv(value_ref, cv_ref, start)
        hidden = (gate / (1.0 + jnp.exp(-gate)) * value).astype(jnp.bfloat16)
        down = jnp.dot(hidden, down_ref[...], preferred_element_type=jnp.float32)
        out_ref[pl.ds(t * 2, 2)] = down.astype(out_ref.dtype).reshape(2, rows, depth)


def feed_forward(pieces, rim, whole, conv_gate, conv_value):
    blocks, rows, depth = pieces.shape
    units = conv_gate.shape[1]
    vmem = pl.BlockSpec(memory_space=pltpu.VMEM)
    return pl.pallas_call(
        feed_forward_kernel,
        out_shape=jax.ShapeDtypeStruct((blocks, rows, depth), jnp.bfloat16),
        in_specs=[vmem, vmem, pl.BlockSpec(memory_space=pl.ANY), vmem, vmem],
        out_specs=vmem,
        scratch_shapes=[
            pltpu.VMEM((2 * units, depth), jnp.bfloat16),
            pltpu.VMEM((units, depth), jnp.bfloat16),
            pltpu.VMEM((RIM + blocks * rows, units), jnp.float32),
            pltpu.VMEM((RIM + blocks * rows, units), jnp.float32),
            pltpu.SemaphoreType.DMA((2, whole.shape[0])),
        ],
        compiler_params=pltpu.CompilerParams(vmem_limit_bytes=56 * 2**20),
        cost_estimate=pl.CostEstimate(flops=9 * 10**9, bytes_accessed=18 * 2**20, transcendentals=0),
        name="feed_forward",
    )(pieces, rim, whole, conv_gate, conv_value)


def reduce_kernel(p_ref, m_ref, out_ref, twin_buf, sum_buf, relay_buf, ring_buf, twin_send, twin_recv, relay_send, relay_recv, ring_send, ring_recv):
    x, core = place_of()
    rows = p_ref.shape[1]
    part = rows // 2
    right = (x + 1) % SIDE
    left = (x + 3) % SIDE
    across = (x + 2) % SIDE
    halves = (slice(0, part), slice(part, rows))

    def twin(chip):
        return remote_copy(
            p_ref.at[2 * chip + 1 - core],
            twin_buf.at[chip],
            twin_send.at[chip],
            twin_recv.at[chip],
            tp=2 * x + 1 - core,
        )

    for chip in (across, right, left, x):
        twin(chip).start()

    def pair_sum(chip, half):
        mine = p_ref[2 * chip + core, halves[half], :].astype(jnp.float32)
        return mine + twin_buf[chip, halves[half], :].astype(jnp.float32)

    def relay(side):
        to = (right, left)[side]
        return remote_copy(
            sum_buf.at[0, halves[side]],
            relay_buf.at[side],
            relay_send.at[side],
            relay_recv.at[side],
            tp=2 * to + core,
        )

    def ring(side, half):
        to = (right, left)[side]
        return remote_copy(
            sum_buf.at[1 + side, halves[half]],
            ring_buf.at[side, halves[half]],
            ring_send.at[side, half],
            ring_recv.at[side, half],
            tp=2 * to + core,
        )

    arrived(twin_buf.at[across], twin_recv.at[across])
    for side in range(2):
        sum_buf[0, halves[side], :] = pair_sum(across, side).astype(jnp.bfloat16)
        relay(side).start()
    for side in range(2):
        to = (right, left)[side]
        arrived(twin_buf.at[to], twin_recv.at[to])
        half = 1 - side
        sum_buf[1 + side, halves[half], :] = pair_sum(to, half).astype(jnp.bfloat16)
        ring(side, half).start()
    arrived(twin_buf.at[x], twin_recv.at[x])
    for side in range(2):
        to = (right, left)[side]
        arrived(relay_buf.at[side], relay_recv.at[side])
        total = pair_sum(to, side) + relay_buf[side].astype(jnp.float32)
        sum_buf[1 + side, halves[side], :] = total.astype(jnp.bfloat16)
        ring(side, side).start()
    for half in range(2):
        total = m_ref[halves[half], :].astype(jnp.float32) + pair_sum(x, half)
        for side in (1 - half, half):
            arrived(ring_buf.at[side, halves[half]], ring_recv.at[side, half])
            total = total + ring_buf[side, halves[half], :].astype(jnp.float32)
        out_ref[halves[half], :] = total.astype(out_ref.dtype)
    for chip in range(SIDE):
        twin(chip).wait_send()
    for side in range(2):
        relay(side).wait_send()
        for half in range(2):
            ring(side, half).wait_send()


def reduce_rows(parts, middle):
    _, rows, depth = parts.shape
    vmem = pl.BlockSpec(memory_space=pltpu.VMEM)
    dma = pltpu.SemaphoreType.DMA
    return pl.pallas_call(
        reduce_kernel,
        out_shape=jax.ShapeDtypeStruct((rows, depth), jnp.bfloat16),
        in_specs=[vmem, vmem],
        out_specs=vmem,
        scratch_shapes=[
            pltpu.VMEM((SIDE, rows, depth), jnp.bfloat16),
            pltpu.VMEM((3, rows, depth), jnp.bfloat16),
            pltpu.VMEM((2, rows // 2, depth), jnp.bfloat16),
            pltpu.VMEM((2, rows, depth), jnp.bfloat16),
            dma((SIDE,)), dma((SIDE,)), dma((2,)), dma((2,)), dma((2, 2)), dma((2, 2)),
        ],
        compiler_params=pltpu.CompilerParams(has_side_effects=True, vmem_limit_bytes=32 * 2**20),
        cost_estimate=pl.CostEstimate(flops=5 * 10**9, bytes_accessed=6 * 2**20, transcendentals=0),
        name="reduce_rows",
    )(parts, middle)


def local(
    queries,
    keys,
    values,
    stick_bias,
    residual,
    out_weight,
    norm_gain,
    gate_weight,
    value_weight,
    down_weight,
    conv_gate,
    conv_value,
):
    rows_here = queries.shape[0]
    bias_rows = stick_bias.reshape(rows_here // CHUNK, CHUNK)
    bias_rows = jnp.pad(bias_rows, ((0, PAD - bias_rows.shape[0]), (0, 0)))
    shared = exchange(queries, keys, values, bias_rows)
    weights = jnp.concatenate([gate_weight.T, value_weight.T, down_weight.T], axis=0)
    weights, shared = lax.optimization_barrier((weights, shared))
    whole = lax.all_gather(weights, "sp", axis=0, tiled=False)
    outs, logs = attention(keys, values, bias_rows, *shared)
    row_heads = combine(*deliver(outs, logs, lax.axis_size("tp")))
    projected = jnp.dot(row_heads, out_weight, preferred_element_type=jnp.float32)
    middle = (residual.astype(jnp.float32) + projected).astype(jnp.bfloat16)
    middle_f = middle.astype(jnp.float32)
    normed = (
        middle_f
        * lax.rsqrt(jnp.mean(middle_f * middle_f, axis=-1, keepdims=True) + EPS)
        * norm_gain
    ).astype(jnp.bfloat16)
    pieces, rim = gather_rows(normed)
    parts = feed_forward(pieces, rim, whole, conv_gate, conv_value)
    return reduce_rows(parts, middle)


def solution(mesh):
    in_specs = (
        P("sp", "tp"),
        P("sp", "tp"),
        P("sp", "tp"),
        P("sp", "tp"),
        P(("sp", "tp"), None),
        P(),
        P(),
        P("sp", "tp"),
        P("sp", "tp"),
        P("sp", "tp"),
        P(None, "tp"),
        P(None, "tp"),
    )
    out_specs = P(("sp", "tp"), None)
    return jax.shard_map(local, mesh=mesh, in_specs=in_specs, out_specs=out_specs, check_vma=False)
```

```python
import jax
import jax.numpy as jnp
from jax import lax
from jax.experimental import pallas as pl
from jax.experimental.pallas import tpu as pltpu
from jax.sharding import PartitionSpec as P

EPS = 1e-06
LOG2E = 1.4426950408889634
NT = (((1,), (1,)), ((), ()))
CHUNK = 256
PAD = 16
SIDE = 4
RIM = 16
VMEM = 67_000_000


def tri_matrix():
    rows = lax.broadcasted_iota(jnp.int32, (CHUNK, CHUNK), 0)
    cols = lax.broadcasted_iota(jnp.int32, (CHUNK, CHUNK), 1)
    return (rows > cols).astype(jnp.bfloat16), rows > cols


def visit_chunk(q, k, v, bias, tri, gone, acc, mask=None):
    scale = 128 ** (-0.5) * LOG2E
    s = lax.dot_general(q, k, NT, preferred_element_type=jnp.float32) * scale + bias
    if mask is not None:
        s = jnp.where(mask, s, -1e30)
    soft = jnp.maximum(jnp.log(1.0 + jnp.exp2(jnp.minimum(s, 126.0))) * LOG2E, s)
    behind = jnp.dot(soft.astype(jnp.bfloat16), tri, preferred_element_type=jnp.float32)
    stick = jnp.exp2((s - soft) - (behind + gone)).astype(jnp.bfloat16)
    acc = acc + jnp.dot(stick, v, preferred_element_type=jnp.float32)
    gone = gone + (behind[:, 0:1] + soft[:, 0:1])
    return gone, acc


def position():
    me = lax.axis_index("sp")
    return me, me // SIDE, me % SIDE


def owners_of(y):
    core = lax.axis_index("tp") % 2
    return 2 * ((y + core) % SIDE), 2 * ((y + core + 2) % SIDE) + 1


def remote_copy(src, dst, send_sem, recv_sem, **where):
    return pltpu.make_async_remote_copy(
        src_ref=src,
        dst_ref=dst,
        send_sem=send_sem,
        recv_sem=recv_sem,
        device_id=where,
        device_id_type=pl.DeviceIdType.MESH,
    )


def arrived(dst, sem):
    pltpu.make_async_copy(dst, dst, sem).wait()


def meet(peers, extra=0):
    barrier = pltpu.get_barrier_semaphore()
    for where in peers:
        pl.semaphore_signal(barrier, inc=1, device_id=where, device_id_type=pl.DeviceIdType.MESH)
    pl.semaphore_wait(barrier, len(peers) + extra)


def exchange_kernel(
    q_ref, k_ref, v_ref, b_ref, qs_ref, ks_ref, vs_ref, bs_ref,
    send_sem, recv_sem, bias_send, bias_recv, q_send, q_recv, own_sem, z_send, z_recv,
):
    me, z, y = position()
    share = q_ref.shape[0] // (2 * SIDE)
    right = (y + 1) % SIDE
    left = (y + 3) % SIDE
    across = (y + 2) % SIDE
    row = z * SIDE
    meet(
        [{"sp": row + (y + d) % SIDE} for d in (1, 2, 3)]
        + [{"sp": (z + d) % SIDE * SIDE + y} for d in (1, 2, 3)]
    )

    def hop(part, src_slot, to, lane):
        src = (k_ref, v_ref)[part] if src_slot is None else (ks_ref, vs_ref)[part].at[src_slot]
        slot = y if src_slot is None else src_slot
        return remote_copy(
            src,
            (ks_ref, vs_ref)[part].at[slot],
            send_sem.at[part, lane],
            recv_sem.at[part, slot],
            sp=row + to,
        )

    def bias_hop(d):
        return remote_copy(
            b_ref, bs_ref.at[y], bias_send.at[d], bias_recv.at[y], sp=row + (y + d) % SIDE
        )

    def q_piece(of, half, act_remote, d):
        src = q_ref.at[pl.ds(pl.multiple_of(owners_of(of)[half] * share, share), share)]
        dst = qs_ref.at[me, pl.ds(half * share, share)]
        if act_remote:
            return remote_copy(
                src, dst, q_send.at[d, half], q_recv.at[me % SIDE, half], sp=row + of
            )
        return pltpu.make_async_copy(src, dst, own_sem.at[half])

    for half in range(2):
        q_piece(y, half, False, 0).start()
    for d in (2, 1, 3):
        for half in range(2):
            q_piece((y + d) % SIDE, half, True, d).start()
        bias_hop(d).start()
    hop(0, None, right, 0).start()
    hop(1, None, left, 0).start()
    hop(1, None, right, 1).start()
    hop(0, None, left, 1).start()

    for half in range(2):
        q_piece(y, half, False, 0).wait()
        for d in (1, 2, 3):
            slot = (y + d) % SIDE
            arrived(qs_ref.at[row + slot, pl.ds(half * share, share)], q_recv.at[slot, half])

    def down_row(dz):
        ours = qs_ref.at[pl.ds(pl.multiple_of(row, SIDE), SIDE)]
        return remote_copy(ours, ours, z_send.at[dz], z_recv.at[z], sp=row - dz * SIDE + y)

    for dz in (2, 3, 1):

        @pl.when(z >= dz)
        def _():
            down_row(dz).start()

    arrived(ks_ref.at[left], recv_sem.at[0, left])
    hop(0, left, right, 2).start()
    arrived(vs_ref.at[right], recv_sem.at[1, right])
    hop(1, right, left, 2).start()
    arrived(vs_ref.at[left], recv_sem.at[1, left])
    arrived(ks_ref.at[right], recv_sem.at[0, right])
    arrived(ks_ref.at[across], recv_sem.at[0, across])
    arrived(vs_ref.at[across], recv_sem.at[1, across])
    for d in (1, 2, 3):
        slot = (y + d) % SIDE
        arrived(bs_ref.at[slot], bias_recv.at[slot])
    for other in range(1, SIDE):

        @pl.when(z < other)
        def _():
            arrived(qs_ref.at[pl.ds(other * SIDE, SIDE)], z_recv.at[other])

    hop(0, None, right, 0).wait_send()
    hop(1, None, left, 0).wait_send()
    hop(1, None, right, 1).wait_send()
    hop(0, None, left, 1).wait_send()
    hop(0, left, right, 2).wait_send()
    hop(1, right, left, 2).wait_send()
    for d in (1, 2, 3):
        bias_hop(d).wait_send()
        for half in range(2):
            q_piece((y + d) % SIDE, half, True, d).wait_send()
    for dz in (1, 2, 3):

        @pl.when(z >= dz)
        def _():
            down_row(dz).wait_send()


def exchange(queries, keys, values, bias_rows):
    rows, head = queries.shape
    anywhere = pl.BlockSpec(memory_space=pl.ANY)
    count = SIDE * SIDE
    dma = pltpu.SemaphoreType.DMA
    return pl.pallas_call(
        exchange_kernel,
        out_shape=(
            jax.ShapeDtypeStruct((count, rows // SIDE, head), jnp.bfloat16),
            jax.ShapeDtypeStruct((SIDE, rows, head), jnp.bfloat16),
            jax.ShapeDtypeStruct((SIDE, rows, head), jnp.bfloat16),
            jax.ShapeDtypeStruct((SIDE,) + bias_rows.shape, jnp.bfloat16),
        ),
        in_specs=[anywhere] * 4,
        out_specs=[anywhere] * 4,
        scratch_shapes=[
            dma((2, 3)), dma((2, SIDE)), dma((SIDE,)), dma((SIDE,)), dma((SIDE, 2)),
            dma((SIDE, 2)), dma((2,)), dma((SIDE,)), dma((SIDE,)),
        ],
        compiler_params=pltpu.CompilerParams(has_side_effects=True, collective_id=0, vmem_limit_bytes=VMEM),
        cost_estimate=pl.CostEstimate(flops=10**10, bytes_accessed=4 * 2**20, transcendentals=0),
        name="exchange",
    )(queries, keys, values, bias_rows)


def attention_kernel(
    k_ref, v_ref, b_ref, qs_ref, ks_ref, vs_ref, bs_ref,
    o_ref, g_ref, q_all, k_all, v_all, b_all, acc_ref, gone_ref, kv_sem, q_sem,
):
    rows, head = k_ref.shape
    quarter = rows // SIDE
    chunks = rows // CHUNK
    _, z, y = position()
    first, second = (owner * (quarter // 2) for owner in owners_of(y))
    tri, _ = tri_matrix()
    own = (k_ref, v_ref, b_ref)
    others = (ks_ref, vs_ref, bs_ref)
    wholes = (k_all, v_all, b_all)

    for slot in range(SIDE - 1, -1, -1):
        for part in range(3):

            @pl.when(slot == y)
            def _():
                pltpu.make_async_copy(own[part], wholes[part].at[slot], kv_sem.at[part, slot]).start()

            @pl.when(slot != y)
            def _():
                pltpu.make_async_copy(
                    others[part].at[slot], wholes[part].at[slot], kv_sem.at[part, slot]
                ).start()

    for slot in range(SIDE * SIDE):
        dst = q_all.at[pl.ds(slot * quarter, quarter)]

        @pl.when(slot // SIDE >= z)
        def _():
            pltpu.make_async_copy(qs_ref.at[slot], dst, q_sem.at[slot]).start()

    for slot in range(SIDE * SIDE):

        @pl.when(slot // SIDE >= z)
        def _():
            dst = q_all.at[pl.ds(slot * quarter, quarter)]
            pltpu.make_async_copy(qs_ref.at[slot], dst, q_sem.at[slot]).wait()

    for slot in range(SIDE):
        for part in range(3):
            pltpu.make_async_copy(
                others[part].at[slot], wholes[part].at[slot], kv_sem.at[part, slot]
            ).wait()

    def finish(group, gone, acc):
        for m in range(SIDE):
            here = slice(m * quarter, (m + 1) * quarter)
            o_ref[group * SIDE + m] = acc[here].astype(o_ref.dtype)
            turned = jnp.broadcast_to(gone[here], (quarter, 128)).T
            for half in range(2):
                g_ref[group * SIDE + m, half] = turned[0:8, half * 128 : (half + 1) * 128]

    acc_ref[...] = jnp.zeros_like(acc_ref)
    gone_ref[...] = jnp.zeros_like(gone_ref)
    for j in range(SIDE - 1, -1, -1):
        low = j * quarter
        size = rows - low
        q = q_all[pl.ds(pl.multiple_of(z * rows + low, quarter), size), :]
        bias = b_all[j].astype(jnp.float32) * LOG2E
        acc = acc_ref[low:, :]
        gone = gone_ref[low:, 0:1]
        row = lax.broadcasted_iota(jnp.int32, (size, CHUNK), 0)
        col = lax.broadcasted_iota(jnp.int32, (size, CHUNK), 1)
        place = row + jnp.where(row < quarter // 2, first, second - quarter // 2)
        for c in range(chunks - 1, -1, -1):
            at = slice(c * CHUNK, (c + 1) * CHUNK)
            mask = (row >= quarter) | (col + c * CHUNK < place)
            gone, acc = visit_chunk(
                q, k_all[j, at, :], v_all[j, at, :], bias[c : c + 1, :], tri, gone, acc, mask
            )
        acc_ref[low:, :] = acc
        gone_ref[low:, :] = jnp.broadcast_to(gone, (size, 128))
    finish(z, gone_ref[:, 0:1], acc_ref[...])

    def group_step(group, carry):
        q = q_all[pl.ds(pl.multiple_of(group * rows, rows), rows), :]

        def block_step(step, state):
            gone, acc = state
            j = SIDE - 1 - step
            bias = b_all[j].astype(jnp.float32) * LOG2E
            for c in range(chunks - 1, -1, -1):
                at = slice(c * CHUNK, (c + 1) * CHUNK)
                gone, acc = visit_chunk(
                    q, k_all[j, at, :], v_all[j, at, :], bias[c : c + 1, :], tri, gone, acc
                )
            return gone, acc

        start = (jnp.zeros((rows, 1), jnp.float32), jnp.zeros((rows, head), jnp.float32))
        gone, acc = lax.fori_loop(0, SIDE, block_step, start)
        finish(group, gone, acc)
        return carry

    lax.fori_loop(z + 1, SIDE, group_step, 0)


def attention(keys, values, bias_rows, q_parts, k_parts, v_parts, b_parts):
    rows, head = keys.shape
    vmem = pl.BlockSpec(memory_space=pltpu.VMEM)
    count = SIDE * SIDE
    return pl.pallas_call(
        attention_kernel,
        out_shape=(
            jax.ShapeDtypeStruct((count, rows // SIDE, head), jnp.bfloat16),
            jax.ShapeDtypeStruct((count, 2, 8, 128), jnp.float32),
        ),
        in_specs=[pl.BlockSpec(memory_space=pltpu.HBM)] * 7,
        out_specs=[vmem, vmem],
        scratch_shapes=[
            pltpu.VMEM((SIDE * rows, head), jnp.bfloat16),
            pltpu.VMEM((SIDE, rows, head), jnp.bfloat16),
            pltpu.VMEM((SIDE, rows, head), jnp.bfloat16),
            pltpu.VMEM((SIDE,) + bias_rows.shape, jnp.bfloat16),
            pltpu.VMEM((rows, head), jnp.float32),
            pltpu.VMEM((rows, 128), jnp.float32),
            pltpu.SemaphoreType.DMA((3, SIDE)),
            pltpu.SemaphoreType.DMA((count,)),
        ],
        compiler_params=pltpu.CompilerParams(vmem_limit_bytes=VMEM),
        cost_estimate=pl.CostEstimate(
            flops=14 * 6 * rows * rows * head, bytes_accessed=4 * 2**20, transcendentals=0
        ),
        name="attention",
    )(keys, values, bias_rows, q_parts, k_parts, v_parts, b_parts)


def deliver_kernel(o_ref, g_ref, os_ref, gs_ref, send_sem, recv_sem):
    me, z, y = position()
    head = lax.axis_index("tp")
    owner_rows = os_ref.shape[2]
    owners = owners_of(y)
    x, core = place_of()
    barrier = pltpu.get_barrier_semaphore()

    def greet(group, carry):
        for source in range(os_ref.shape[0]):
            row = (x - source % 2 - 2 * core + 2 * SIDE) % SIDE
            pl.semaphore_signal(
                barrier,
                inc=1,
                device_id={"sp": group * SIDE + row, "tp": source},
                device_id_type=pl.DeviceIdType.MESH,
            )
        return carry

    lax.fori_loop(0, z + 1, greet, 0)
    pl.semaphore_wait(barrier, 2 * (SIDE * SIDE - z * SIDE))

    def pieces(block, half):
        src = o_ref.at[block, pl.ds(half * owner_rows, owner_rows)]
        return ((src, os_ref), (g_ref.at[block, half], gs_ref))

    def remote(block, half, part):
        src, dst = pieces(block, half)[part]
        return pltpu.make_async_remote_copy(
            src_ref=src,
            dst_ref=dst.at[head, z],
            send_sem=send_sem.at[part, block, half],
            recv_sem=recv_sem.at[part, head, z],
            device_id={"sp": block, "tp": owners[half]},
            device_id_type=pl.DeviceIdType.MESH,
        )

    def local_copy(block, half, part):
        src, dst = pieces(block, half)[part]
        return pltpu.make_async_copy(src, dst.at[head, z], recv_sem.at[part, head, z])

    def is_me(block, half):
        return (block == me) & (owners[half] == head)

    def send(block, carry):
        for half in range(2):

            @pl.when(is_me(block, half))
            def _():
                for part in range(2):
                    local_copy(block, half, part).start()

            @pl.when(jnp.logical_not(is_me(block, half)))
            def _():
                for part in range(2):
                    remote(block, half, part).start()

        return carry

    lax.fori_loop(z * SIDE, SIDE * SIDE, send, 0)

    def take(group, carry):
        for h in range(os_ref.shape[0]):
            for part in range(2):
                dst = (os_ref, gs_ref)[part].at[h, group]
                pltpu.make_async_copy(dst, dst, recv_sem.at[part, h, group]).wait()
        return carry

    lax.fori_loop(0, z + 1, take, 0)

    def sent(block, carry):
        for half in range(2):

            @pl.when(jnp.logical_not(is_me(block, half)))
            def _():
                for part in range(2):
                    remote(block, half, part).wait_send()

        return carry

    lax.fori_loop(z * SIDE, SIDE * SIDE, sent, 0)


def deliver(outs, logs, heads):
    count, quarter, head = outs.shape
    vmem = pl.BlockSpec(memory_space=pltpu.VMEM)
    return pl.pallas_call(
        deliver_kernel,
        out_shape=(
            jax.ShapeDtypeStruct((heads, SIDE, quarter // 2, head), jnp.bfloat16),
            jax.ShapeDtypeStruct((heads, SIDE, 8, 128), jnp.float32),
        ),
        in_specs=[vmem, vmem],
        out_specs=[vmem, vmem],
        scratch_shapes=[
            pltpu.SemaphoreType.DMA((2, count, 2)),
            pltpu.SemaphoreType.DMA((2, heads, SIDE)),
        ],
        compiler_params=pltpu.CompilerParams(has_side_effects=True, collective_id=1, vmem_limit_bytes=VMEM),
        cost_estimate=pl.CostEstimate(flops=5 * 10**9, bytes_accessed=4 * 2**20, transcendentals=0),
        name="deliver",
    )(outs, logs)


def combine(parts, logs):
    group = lax.axis_index("sp") // SIDE
    valid = jnp.arange(SIDE) <= group
    left = jnp.where(valid[None, :, None], logs[:, :, 0, :], 0.0)
    later = jnp.flip(jnp.cumsum(jnp.flip(left, 1), axis=1), 1) - left
    weight = jnp.where(valid[None, :, None], jnp.exp2(-later), 0.0)
    terms = jnp.where(valid[None, :, None, None], parts.astype(jnp.float32), 0.0)
    total = jnp.sum(terms * weight[..., None], axis=1)
    return total.transpose(1, 0, 2).reshape(total.shape[1], -1).astype(jnp.bfloat16)


def place_of():
    me = lax.axis_index("tp")
    return me // 2, me % 2


def feed_forward_kernel(
    n_ref, m_ref, w_ref, cg_ref, cv_ref, out_ref,
    all_ref, rim_ref, up_ref, down_ref, gate_ref, value_ref, p_ref, twin_buf, sum_buf, relay_buf,
    ring_buf, w_sem, ring_send, ring_recv, twin_send, twin_recv, rim_send, rim_recv, own_sem,
    pair_send, pair_recv, relay_send, relay_recv, back_send, back_recv,
):
    x, core = place_of()
    block = lax.axis_index("sp")
    rows, depth = n_ref.shape
    part = rows // 2
    tile = 2 * rows
    units = down_ref.shape[0]
    shards = w_ref.shape[0]
    deep = depth // shards
    right = (x + 1) % SIDE
    left = (x + 3) % SIDE
    across = (x + 2) % SIDE
    other = 2 * x + 1 - core
    halves = (slice(0, part), slice(part, rows))

    def weight_copies(k):
        at = slice(k * deep, (k + 1) * deep)
        return (
            pltpu.make_async_copy(
                w_ref.at[k, pl.ds(0, 2 * units)], up_ref.at[:, at], w_sem.at[0, k]
            ),
            pltpu.make_async_copy(
                w_ref.at[k, pl.ds(2 * units, units)], down_ref.at[:, at], w_sem.at[1, k]
            ),
        )

    for k in range(shards):
        for copy in weight_copies(k):
            copy.start()

    def spot(chip, half, of_core):
        return all_ref.at[2 * chip + of_core, pl.ds(half * part, part)]

    def ring(chip, half, to, lane):
        src = n_ref.at[pl.ds(half * part, part)] if chip is None else spot(chip, half, core)
        chip = x if chip is None else chip
        return remote_copy(
            src,
            spot(chip, half, core),
            ring_send.at[lane, half],
            ring_recv.at[chip, half],
            tp=2 * to + core,
        )

    def twin(chip, half):
        src = n_ref.at[pl.ds(half * part, part)] if chip is None else spot(chip, half, core)
        chip = x if chip is None else chip
        return remote_copy(
            src, spot(chip, half, core), twin_send.at[chip, half], twin_recv.at[chip, half], tp=other
        )

    def rim(to):
        return remote_copy(
            n_ref.at[pl.ds(rows - RIM, RIM)], rim_ref, rim_send.at[to], rim_recv, sp=block + 1, tp=to
        )

    last = (x == SIDE - 1) & (core == 1) & (block < SIDE * SIDE - 1)
    barrier = pltpu.get_barrier_semaphore()

    @pl.when(block > 0)
    def _():
        pl.semaphore_signal(
            barrier,
            inc=1,
            device_id={"sp": block - 1, "tp": 2 * SIDE - 1},
            device_id_type=pl.DeviceIdType.MESH,
        )

    meet(
        [{"tp": 2 * right + core}, {"tp": 2 * left + core}, {"tp": other}],
        jnp.where(last, 2 * SIDE, 0),
    )
    own = pltpu.make_async_copy(n_ref, all_ref.at[2 * x + core], own_sem)
    ring(None, 0, right, 0).start()
    ring(None, 1, left, 1).start()
    ring(None, 1, right, 0).start()
    ring(None, 0, left, 1).start()
    own.start()
    for half in range(2):
        twin(None, half).start()

    @pl.when(last)
    def _():
        for to in range(2 * SIDE):
            rim(to).start()

    def up(rows_in, which):
        w = up_ref[which * units : (which + 1) * units, :]
        return lax.dot_general(rows_in, w, NT, preferred_element_type=jnp.float32)

    def project_up(chip):
        rows_in = all_ref[pl.ds(2 * chip, 2)].reshape(tile, depth)
        for which, ref in enumerate((gate_ref, value_ref)):
            ref[pl.ds(pl.multiple_of(chip * tile + RIM, RIM), tile), :] = up(rows_in, which)

    def conv(ref, taps, chip):
        window = ref[pl.ds(pl.multiple_of(chip * tile, tile), tile + RIM), :]
        return (
            taps[0:1, :] * window[RIM - 2 : RIM - 2 + tile]
            + taps[1:2, :] * window[RIM - 1 : RIM - 1 + tile]
            + taps[2:3, :] * window[RIM : RIM + tile]
        )

    def project_down(chip):
        gate = conv(gate_ref, cg_ref, chip)
        value = conv(value_ref, cv_ref, chip)
        hidden = (gate / (1.0 + jnp.exp(-gate)) * value).astype(jnp.bfloat16)
        down = jnp.dot(hidden, down_ref[...], preferred_element_type=jnp.float32)
        p_ref[pl.ds(2 * chip, 2)] = down.astype(p_ref.dtype).reshape(2, rows, depth)

    def twin_arrived(chip):
        for half in range(2):
            arrived(spot(chip, half, 1 - core), twin_recv.at[chip, half])

    for k in range(shards):
        weight_copies(k)[0].wait()
    own.wait()
    twin_arrived(x)
    project_up(x)
    arrived(spot(left, 0, core), ring_recv.at[left, 0])
    ring(left, 0, right, 2).start()
    twin(left, 0).start()
    arrived(spot(right, 1, core), ring_recv.at[right, 1])
    ring(right, 1, left, 2).start()
    twin(right, 1).start()

    @pl.when(block > 0)
    def _():
        arrived(rim_ref, rim_recv)
        for which, ref in enumerate((gate_ref, value_ref)):
            ref[0:RIM, :] = up(rim_ref[...], which)

    @pl.when(block == 0)
    def _():
        for ref in (gate_ref, value_ref):
            ref[0:RIM, :] = jnp.zeros((RIM, units), jnp.float32)

    for chip, half in ((left, 1), (right, 0)):
        arrived(spot(chip, half, core), ring_recv.at[chip, half])
        twin(chip, half).start()
    twin_arrived(right)
    project_up(right)
    twin_arrived(left)
    project_up(left)
    for half in range(2):
        arrived(spot(across, half, core), ring_recv.at[across, half])
        twin(across, half).start()
    for k in range(shards):
        weight_copies(k)[1].wait()

    def pair(chip):
        return remote_copy(
            p_ref.at[2 * chip + 1 - core],
            twin_buf.at[chip],
            pair_send.at[chip],
            pair_recv.at[chip],
            tp=other,
        )

    def pair_sum(chip, half):
        mine = p_ref[2 * chip + core, halves[half], :].astype(jnp.float32)
        return mine + twin_buf[chip, halves[half], :].astype(jnp.float32)

    def relay(side):
        return remote_copy(
            sum_buf.at[0, halves[side]],
            relay_buf.at[side],
            relay_send.at[side],
            relay_recv.at[side],
            tp=2 * (right, left)[side] + core,
        )

    def back(side, half):
        return remote_copy(
            sum_buf.at[1 + side, halves[half]],
            ring_buf.at[side, halves[half]],
            back_send.at[side, half],
            back_recv.at[side, half],
            tp=2 * (right, left)[side] + core,
        )

    def direct(side):
        to = (right, left)[side]
        half = 1 - side
        arrived(twin_buf.at[to], pair_recv.at[to])
        sum_buf[1 + side, halves[half], :] = pair_sum(to, half).astype(jnp.bfloat16)
        back(side, half).start()

    project_down(right)
    pair(right).start()
    project_down(x)
    pair(x).start()
    direct(0)
    twin_arrived(across)
    project_up(across)
    project_down(across)
    pair(across).start()
    arrived(twin_buf.at[across], pair_recv.at[across])
    for side in range(2):
        sum_buf[0, halves[side], :] = pair_sum(across, side).astype(jnp.bfloat16)
        relay(side).start()
    project_down(left)
    pair(left).start()
    direct(1)
    arrived(twin_buf.at[x], pair_recv.at[x])
    for side in range(2):
        to = (right, left)[side]
        arrived(relay_buf.at[side], relay_recv.at[side])
        total = pair_sum(to, side) + relay_buf[side].astype(jnp.float32)
        sum_buf[1 + side, halves[side], :] = total.astype(jnp.bfloat16)
        back(side, side).start()
    for half in range(2):
        total = m_ref[halves[half], :].astype(jnp.float32) + pair_sum(x, half)
        for side in (1 - half, half):
            arrived(ring_buf.at[side, halves[half]], back_recv.at[side, half])
            total = total + ring_buf[side, halves[half], :].astype(jnp.float32)
        out_ref[halves[half], :] = total.astype(out_ref.dtype)

    for half in range(2):
        ring(None, half, right, 0).wait_send()
        ring(None, half, left, 1).wait_send()
        twin(None, half).wait_send()
        for chip in (left, right, across):
            twin(chip, half).wait_send()
    ring(left, 0, right, 2).wait_send()
    ring(right, 1, left, 2).wait_send()

    @pl.when(last)
    def _():
        for to in range(2 * SIDE):
            rim(to).wait_send()

    for chip in range(SIDE):
        pair(chip).wait_send()
    for side in range(2):
        relay(side).wait_send()
        for half in range(2):
            back(side, half).wait_send()


def feed_forward(normed, middle, whole, conv_gate, conv_value):
    rows, depth = normed.shape
    units = conv_gate.shape[1]
    total = 2 * SIDE * rows
    vmem = pl.BlockSpec(memory_space=pltpu.VMEM)
    dma = pltpu.SemaphoreType.DMA
    bf16 = jnp.bfloat16
    return pl.pallas_call(
        feed_forward_kernel,
        out_shape=jax.ShapeDtypeStruct((rows, depth), bf16),
        in_specs=[vmem, vmem, pl.BlockSpec(memory_space=pl.ANY), vmem, vmem],
        out_specs=vmem,
        scratch_shapes=[
            pltpu.VMEM((2 * SIDE, rows, depth), bf16),
            pltpu.VMEM((RIM, depth), bf16),
            pltpu.VMEM((2 * units, depth), bf16),
            pltpu.VMEM((units, depth), bf16),
            pltpu.VMEM((RIM + total, units), jnp.float32),
            pltpu.VMEM((RIM + total, units), jnp.float32),
            pltpu.VMEM((2 * SIDE, rows, depth), bf16),
            pltpu.VMEM((SIDE, rows, depth), bf16),
            pltpu.VMEM((3, rows, depth), bf16),
            pltpu.VMEM((2, rows // 2, depth), bf16),
            pltpu.VMEM((2, rows, depth), bf16),
            dma((2, whole.shape[0])),
            dma((3, 2)), dma((SIDE, 2)), dma((SIDE, 2)), dma((SIDE, 2)), dma((2 * SIDE,)), dma(()), dma(()),
            dma((SIDE,)), dma((SIDE,)), dma((2,)), dma((2,)), dma((2, 2)), dma((2, 2)),
        ],
        compiler_params=pltpu.CompilerParams(
            has_side_effects=True, collective_id=2, vmem_limit_bytes=VMEM
        ),
        cost_estimate=pl.CostEstimate(
            flops=9 * 10**9, bytes_accessed=12 * 2**20, transcendentals=0
        ),
        name="feed_forward",
    )(normed, middle, whole, conv_gate, conv_value)


def local(
    queries,
    keys,
    values,
    stick_bias,
    residual,
    out_weight,
    norm_gain,
    gate_weight,
    value_weight,
    down_weight,
    conv_gate,
    conv_value,
):
    rows_here = queries.shape[0]
    bias_rows = stick_bias.reshape(rows_here // CHUNK, CHUNK)
    bias_rows = jnp.pad(bias_rows, ((0, PAD - bias_rows.shape[0]), (0, 0)))
    shared = exchange(queries, keys, values, bias_rows)
    weights = jnp.concatenate([gate_weight.T, value_weight.T, down_weight.T], axis=0)
    weights, shared = lax.optimization_barrier((weights, shared))
    whole = lax.all_gather(weights, "sp", axis=0, tiled=False)
    outs, logs = attention(keys, values, bias_rows, *shared)
    row_heads = combine(*deliver(outs, logs, lax.axis_size("tp")))
    projected = jnp.dot(row_heads, out_weight, preferred_element_type=jnp.float32)
    middle = (residual.astype(jnp.float32) + projected).astype(jnp.bfloat16)
    middle_f = middle.astype(jnp.float32)
    normed = (
        middle_f
        * lax.rsqrt(jnp.mean(middle_f * middle_f, axis=-1, keepdims=True) + EPS)
        * norm_gain
    ).astype(jnp.bfloat16)
    return feed_forward(normed, middle, whole, conv_gate, conv_value)


def solution(mesh):
    in_specs = (
        P("sp", "tp"),
        P("sp", "tp"),
        P("sp", "tp"),
        P("sp", "tp"),
        P(("sp", "tp"), None),
        P(),
        P(),
        P("sp", "tp"),
        P("sp", "tp"),
        P("sp", "tp"),
        P(None, "tp"),
        P(None, "tp"),
    )
    out_specs = P(("sp", "tp"), None)
    return jax.shard_map(local, mesh=mesh, in_specs=in_specs, out_specs=out_specs, check_vma=False)
```

```python
import jax
import jax.numpy as jnp
from jax import lax
from jax.experimental import pallas as pl
from jax.experimental.pallas import tpu as pltpu
from jax.sharding import PartitionSpec as P

EPS = 1e-06
LOG2E = 1.4426950408889634
NT = (((1,), (1,)), ((), ()))
CHUNK = 256
PAD = 16
SIDE = 4
RIM = 16
VMEM = 67_000_000


def tri_matrix():
    rows = lax.broadcasted_iota(jnp.int32, (CHUNK, CHUNK), 0)
    cols = lax.broadcasted_iota(jnp.int32, (CHUNK, CHUNK), 1)
    return (rows > cols).astype(jnp.bfloat16), rows > cols


def visit_chunk(q, k, v, bias, tri, gone, acc, mask=None):
    scale = 128 ** (-0.5) * LOG2E
    s = lax.dot_general(q, k, NT, preferred_element_type=jnp.float32) * scale + bias
    if mask is not None:
        s = jnp.where(mask, s, -1e30)
    soft = jnp.maximum(jnp.log(1.0 + jnp.exp2(jnp.minimum(s, 126.0))) * LOG2E, s)
    behind = jnp.dot(soft.astype(jnp.bfloat16), tri, preferred_element_type=jnp.float32)
    stick = jnp.exp2((s - soft) - (behind + gone)).astype(jnp.bfloat16)
    acc = acc + jnp.dot(stick, v, preferred_element_type=jnp.float32)
    gone = gone + (behind[:, 0:1] + soft[:, 0:1])
    return gone, acc


def position():
    me = lax.axis_index("sp")
    return me, me // SIDE, me % SIDE


def owners_of(y):
    core = lax.axis_index("tp") % 2
    return 2 * ((y + core) % SIDE), 2 * ((y + core + 2) % SIDE) + 1


def place_of():
    me = lax.axis_index("tp")
    return me // 2, me % 2


def remote_copy(src, dst, send_sem, recv_sem, **where):
    return pltpu.make_async_remote_copy(
        src_ref=src,
        dst_ref=dst,
        send_sem=send_sem,
        recv_sem=recv_sem,
        device_id=where,
        device_id_type=pl.DeviceIdType.MESH,
    )


def arrived(dst, sem):
    pltpu.make_async_copy(dst, dst, sem).wait()


def meet(peers, extra=0):
    barrier = pltpu.get_barrier_semaphore()
    for where in peers:
        pl.semaphore_signal(barrier, inc=1, device_id=where, device_id_type=pl.DeviceIdType.MESH)
    pl.semaphore_wait(barrier, len(peers) + extra)


def attend_kernel(
    q_ref, k_ref, v_ref, b_ref, w_ref, os_ref, gs_ref, whole_ref,
    q_all, k_all, v_all, b_all, o_buf, g_buf, acc_ref, gone_ref,
    kv_send, kv_recv, kv_own, bias_send, bias_recv, bias_own, q_send, q_recv, q_own, z_send, z_recv,
    w1_send, w1_relay, w2_send, w2_relay, w_recv, w_own, o_send, o_recv,
):
    me, z, y = position()
    x, core = place_of()
    head = lax.axis_index("tp")
    rows, width = k_ref.shape
    quarter = rows // SIDE
    share = quarter // 2
    chunks = rows // CHUNK
    right = (y + 1) % SIDE
    left = (y + 3) % SIDE
    across = (y + 2) % SIDE
    row = z * SIDE
    owners = owners_of(y)
    tri, _ = tri_matrix()

    barrier = pltpu.get_barrier_semaphore()

    def greet(group, carry):
        for source in range(os_ref.shape[0]):
            of = (x - source % 2 - 2 * core + 2 * SIDE) % SIDE
            pl.semaphore_signal(
                barrier,
                inc=1,
                device_id={"sp": group * SIDE + of, "tp": source},
                device_id_type=pl.DeviceIdType.MESH,
            )
        return carry

    lax.fori_loop(0, z + 1, greet, 0)
    meet(
        [{"sp": row + (y + d) % SIDE} for d in (1, 2, 3)]
        + [{"sp": (z + d) % SIDE * SIDE + y} for d in (1, 2, 3)],
        2 * (SIDE * SIDE - row),
    )

    def hop(part, src_slot, to, lane):
        src = (k_ref, v_ref)[part] if src_slot is None else (k_all, v_all)[part].at[src_slot]
        slot = y if src_slot is None else src_slot
        return remote_copy(
            src,
            (k_all, v_all)[part].at[slot],
            kv_send.at[part, lane],
            kv_recv.at[part, slot],
            sp=row + to,
        )

    def kv_mine(part):
        return pltpu.make_async_copy(
            (k_ref, v_ref)[part], (k_all, v_all)[part].at[y], kv_own.at[part]
        )

    def bias_hop(d):
        return remote_copy(
            b_ref, b_all.at[y], bias_send.at[d], bias_recv.at[y], sp=row + (y + d) % SIDE
        )

    def q_source(of, half):
        return q_ref.at[pl.ds(pl.multiple_of(owners_of(of)[half] * share, share), share)]

    def q_mine(half):
        return pltpu.make_async_copy(
            q_source(y, half), q_all.at[me, pl.ds(half * share, share)], q_own.at[half]
        )

    def q_piece(d, half):
        of = (y + d) % SIDE
        return remote_copy(
            q_source(of, half),
            q_all.at[me, pl.ds(half * share, share)],
            q_send.at[d, half],
            q_recv.at[y, half],
            sp=row + of,
        )

    def q_down(dz):
        ours = q_all.at[pl.ds(pl.multiple_of(row, SIDE), SIDE)]
        return remote_copy(ours, ours, z_send.at[dz], z_recv.at[z], sp=row - dz * SIDE + y)

    bulk = w_ref.shape[0] // 2
    piece = bulk // 2
    steps = (0, 3, 1, 2)

    def w_axes(part):
        return (y, z) if part == 0 else (z, y)

    def w_index(part, c1, c2):
        return c2 * SIDE + c1 if part == 0 else c1 * SIDE + c2

    def w_rows(part, half):
        return pl.ds(part * bulk + half * piece, piece)

    def w_copy(part, half, c1, c2, own, to1, to2, send):
        slot = w_index(part, c1, c2)
        spot = whole_ref.at[slot, w_rows(part, half)]
        src = w_ref.at[w_rows(part, half)] if own else spot
        return remote_copy(
            src, spot, send, w_recv.at[part, slot, half], sp=w_index(part, to1, to2)
        )

    def w_first(part, way, half):
        c1, c2 = w_axes(part)
        to = (c1 + (1, 3)[way]) % SIDE
        return w_copy(part, half, c1, c2, True, to, c2, w1_send.at[part, way, half])

    def w_first_relay(part, way):
        c1, c2 = w_axes(part)
        source = (c1 + (3, 1)[way]) % SIDE
        to = (c1 + (1, 3)[way]) % SIDE
        return w_copy(part, way, source, c2, False, to, c2, w1_relay.at[part, way])

    def w_second(part, k, way, half):
        c1, c2 = w_axes(part)
        to = (c2 + (1, 3)[way]) % SIDE
        source = (c1 + steps[k]) % SIDE
        return w_copy(part, half, source, c2, k == 0, c1, to, w2_send.at[part, k, way, half])

    def w_second_relay(part, k, way):
        c1, c2 = w_axes(part)
        source = (c2 + (3, 1)[way]) % SIDE
        to = (c2 + (1, 3)[way]) % SIDE
        return w_copy(
            part, way, (c1 + steps[k]) % SIDE, source, False, c1, to, w2_relay.at[part, k, way]
        )

    def w_take(part, half, c1, c2):
        slot = w_index(part, c1, c2)
        arrived(whole_ref.at[slot, w_rows(part, half)], w_recv.at[part, slot, half])

    def w_mine():
        return pltpu.make_async_copy(w_ref, whole_ref.at[me], w_own)

    def w_stage(stage):
        for part in range(2):
            c1, c2 = w_axes(part)
            low, high, far = ((c1 + d) % SIDE for d in (3, 1, 2))
            if stage == 0:
                for half in range(2):
                    w_first(part, 0, half).start()
                    w_first(part, 1, 1 - half).start()
            elif stage == 1:
                for half in range(2):
                    w_second(part, 0, 0, half).start()
                    w_second(part, 0, 1, 1 - half).start()
            elif stage == 2:
                w_take(part, 0, low, c2)
                w_first_relay(part, 0).start()
                w_take(part, 1, high, c2)
                w_first_relay(part, 1).start()
            elif stage == 3:
                w_take(part, 1, low, c2)
                w_take(part, 0, high, c2)
                for k in (1, 2):
                    for half in range(2):
                        w_second(part, k, 0, half).start()
                        w_second(part, k, 1, 1 - half).start()
            elif stage == 4:
                for half in range(2):
                    w_take(part, half, far, c2)
                for half in range(2):
                    w_second(part, 3, 0, half).start()
                    w_second(part, 3, 1, 1 - half).start()
            elif stage < 9:
                k = stage - 5
                for way in range(2):
                    w_take(part, way, (c1 + steps[k]) % SIDE, (c2 + (3, 1)[way]) % SIDE)
                    w_second_relay(part, k, way).start()
            else:
                for k in range(SIDE):
                    source = (c1 + steps[k]) % SIDE
                    w_take(part, 1, source, (c2 + 3) % SIDE)
                    w_take(part, 0, source, (c2 + 1) % SIDE)
                    for half in range(2):
                        w_take(part, half, source, (c2 + 2) % SIDE)

    def w_sent():
        for part in range(2):
            for way in range(2):
                w_first_relay(part, way).wait_send()
                for half in range(2):
                    w_first(part, way, half).wait_send()
                for k in range(SIDE):
                    w_second_relay(part, k, way).wait_send()
                    for half in range(2):
                        w_second(part, k, way, half).wait_send()

    def out_pieces(block, half):
        src = o_buf.at[block, pl.ds(half * share, share)]
        return ((src, os_ref), (g_buf.at[block, half], gs_ref))

    def out_remote(block, half, part):
        src, dst = out_pieces(block, half)[part]
        return remote_copy(
            src,
            dst.at[head, z],
            o_send.at[part, block, half],
            o_recv.at[part, head, z],
            sp=block,
            tp=owners[half],
        )

    def out_local(block, half, part):
        src, dst = out_pieces(block, half)[part]
        return pltpu.make_async_copy(src, dst.at[head, z], o_recv.at[part, head, z])

    def for_outs(group, act, act_local):
        for m in range(SIDE):
            block = group * SIDE + m
            for half in range(2):
                mine = (block == me) & (owners[half] == head)
                if act_local is not None:

                    @pl.when(mine)
                    def _():
                        for part in range(2):
                            act_local(out_local(block, half, part))

                @pl.when(jnp.logical_not(mine))
                def _():
                    for part in range(2):
                        act(out_remote(block, half, part))

    def finish(group):
        acc = acc_ref[...]
        gone = gone_ref[...]
        for m in range(SIDE):
            here = slice(m * quarter, (m + 1) * quarter)
            o_buf[group * SIDE + m] = acc[here].astype(o_buf.dtype)
            turned = gone[here].T
            for half in range(2):
                g_buf[group * SIDE + m, half] = turned[0:8, half * 128 : (half + 1) * 128]
        for_outs(group, lambda copy: copy.start(), lambda copy: copy.start())

    for half in range(2):
        q_mine(half).start()
    for d in (2, 1, 3):
        for half in range(2):
            q_piece(d, half).start()
        bias_hop(d).start()
    hop(0, None, right, 0).start()
    hop(1, None, left, 0).start()
    hop(1, None, right, 1).start()
    hop(0, None, left, 1).start()
    for part in range(2):
        kv_mine(part).start()
    bias_mine = pltpu.make_async_copy(b_ref, b_all.at[y], bias_own)
    bias_mine.start()
    for half in range(2):
        q_mine(half).wait()
        for d in (1, 2, 3):
            slot = (y + d) % SIDE
            arrived(q_all.at[row + slot, pl.ds(half * share, share)], q_recv.at[slot, half])
    for dz in (2, 3, 1):

        @pl.when(z >= dz)
        def _():
            q_down(dz).start()

    arrived(k_all.at[left], kv_recv.at[0, left])
    hop(0, left, right, 2).start()
    arrived(v_all.at[right], kv_recv.at[1, right])
    hop(1, right, left, 2).start()
    w_stage(0)
    w_stage(1)
    w_mine().start()
    arrived(v_all.at[left], kv_recv.at[1, left])
    arrived(k_all.at[right], kv_recv.at[0, right])
    arrived(k_all.at[across], kv_recv.at[0, across])
    arrived(v_all.at[across], kv_recv.at[1, across])
    for part in range(2):
        kv_mine(part).wait()
    bias_mine.wait()
    for d in (1, 2, 3):
        slot = (y + d) % SIDE
        arrived(b_all.at[slot], bias_recv.at[slot])

    first, second = (owner * share for owner in owners)
    acc_ref[...] = jnp.zeros_like(acc_ref)
    gone_ref[...] = jnp.zeros_like(gone_ref)
    for j in range(SIDE - 1, -1, -1):
        low = j * quarter
        size = rows - low
        q = q_all[pl.ds(row + j, SIDE - j)].reshape(size, width)
        bias = b_all[j].astype(jnp.float32) * LOG2E
        acc = acc_ref[low:, :]
        gone = gone_ref[low:, 0:1]
        at_row = lax.broadcasted_iota(jnp.int32, (size, CHUNK), 0)
        col = lax.broadcasted_iota(jnp.int32, (size, CHUNK), 1)
        place = at_row + jnp.where(at_row < share, first, second - share)
        for c in range(chunks - 1, -1, -1):
            at = slice(c * CHUNK, (c + 1) * CHUNK)
            mask = (at_row >= quarter) | (col + c * CHUNK < place)
            gone, acc = visit_chunk(
                q, k_all[j, at, :], v_all[j, at, :], bias[c : c + 1, :], tri, gone, acc, mask
            )
        acc_ref[low:, :] = acc
        gone_ref[low:, :] = jnp.broadcast_to(gone, (size, 128))
    finish(z)
    w_stage(2)
    for other in range(1, SIDE):

        @pl.when(z < other)
        def _():
            arrived(q_all.at[pl.ds(other * SIDE, SIDE)], z_recv.at[other])

    def step(s, carry):
        group = z + 1 + s // SIDE
        j = SIDE - 1 - s % SIDE

        @pl.when(group < SIDE)
        def _():
            @pl.when(j == SIDE - 1)
            def _():
                acc_ref[...] = jnp.zeros_like(acc_ref)
                gone_ref[...] = jnp.zeros_like(gone_ref)

            q = q_all[pl.ds(group * SIDE, SIDE)].reshape(rows, width)
            bias = b_all[j].astype(jnp.float32) * LOG2E
            gone = gone_ref[:, 0:1]
            acc = acc_ref[...]
            for c in range(chunks - 1, -1, -1):
                at = slice(c * CHUNK, (c + 1) * CHUNK)
                gone, acc = visit_chunk(
                    q, k_all[j, at, :], v_all[j, at, :], bias[c : c + 1, :], tri, gone, acc
                )
            acc_ref[...] = acc
            gone_ref[...] = jnp.broadcast_to(gone, (rows, 128))

            @pl.when(j == 0)
            def _():
                finish(group)

        for stage, after in ((3, 0), (4, 1), (5, 2), (6, 4), (7, 6), (8, 8)):

            @pl.when(s == after)
            def _():
                w_stage(stage)

        return carry

    lax.fori_loop(0, (SIDE - 1) * SIDE, step, 0)

    def take(group, carry):
        for h in range(os_ref.shape[0]):
            for part in range(2):
                arrived((os_ref, gs_ref)[part].at[h, group], o_recv.at[part, h, group])
        return carry

    lax.fori_loop(0, z + 1, take, 0)
    w_stage(9)
    w_mine().wait()

    def sent(group, carry):
        for_outs(group, lambda copy: copy.wait_send(), None)
        return carry

    lax.fori_loop(z, SIDE, sent, 0)
    w_sent()
    hop(0, None, right, 0).wait_send()
    hop(1, None, left, 0).wait_send()
    hop(1, None, right, 1).wait_send()
    hop(0, None, left, 1).wait_send()
    hop(0, left, right, 2).wait_send()
    hop(1, right, left, 2).wait_send()
    for d in (1, 2, 3):
        bias_hop(d).wait_send()
        for half in range(2):
            q_piece(d, half).wait_send()
    for dz in (1, 2, 3):

        @pl.when(z >= dz)
        def _():
            q_down(dz).wait_send()


def attend(queries, keys, values, bias_rows, weights, heads):
    rows, width = queries.shape
    anywhere = pl.BlockSpec(memory_space=pl.ANY)
    vmem = pl.BlockSpec(memory_space=pltpu.VMEM)
    count = SIDE * SIDE
    quarter = rows // SIDE
    dma = pltpu.SemaphoreType.DMA
    bf16 = jnp.bfloat16
    return pl.pallas_call(
        attend_kernel,
        out_shape=(
            jax.ShapeDtypeStruct((heads, SIDE, quarter // 2, width), bf16),
            jax.ShapeDtypeStruct((heads, SIDE, 8, 128), jnp.float32),
            jax.ShapeDtypeStruct((count,) + weights.shape, bf16),
        ),
        in_specs=[anywhere, anywhere, anywhere, vmem, anywhere],
        out_specs=[vmem, vmem, anywhere],
        scratch_shapes=[
            pltpu.VMEM((count, quarter, width), bf16),
            pltpu.VMEM((SIDE, rows, width), bf16),
            pltpu.VMEM((SIDE, rows, width), bf16),
            pltpu.VMEM((SIDE,) + bias_rows.shape, bf16),
            pltpu.VMEM((count, quarter, width), bf16),
            pltpu.VMEM((count, 2, 8, 128), jnp.float32),
            pltpu.VMEM((rows, width), jnp.float32),
            pltpu.VMEM((rows, 128), jnp.float32),
            dma((2, 3)), dma((2, SIDE)), dma((2,)), dma((SIDE,)), dma((SIDE,)), dma(()),
            dma((SIDE, 2)), dma((SIDE, 2)), dma((2,)), dma((SIDE,)), dma((SIDE,)),
            dma((2, 2, 2)), dma((2, 2)), dma((2, SIDE, 2, 2)), dma((2, SIDE, 2)),
            dma((2, count, 2)), dma(()), dma((2, count, 2)), dma((2, heads, SIDE)),
        ],
        compiler_params=pltpu.CompilerParams(
            has_side_effects=True, collective_id=0, vmem_limit_bytes=VMEM
        ),
        cost_estimate=pl.CostEstimate(
            flops=14 * 6 * rows * rows * width, bytes_accessed=12 * 2**20, transcendentals=0
        ),
        name="attend",
    )(queries, keys, values, bias_rows, weights)


def combine(parts, logs):
    group = lax.axis_index("sp") // SIDE
    valid = jnp.arange(SIDE) <= group
    left = jnp.where(valid[None, :, None], logs[:, :, 0, :], 0.0)
    later = jnp.flip(jnp.cumsum(jnp.flip(left, 1), axis=1), 1) - left
    weight = jnp.where(valid[None, :, None], jnp.exp2(-later), 0.0)
    terms = jnp.where(valid[None, :, None, None], parts.astype(jnp.float32), 0.0)
    total = jnp.sum(terms * weight[..., None], axis=1)
    return total.transpose(1, 0, 2).reshape(total.shape[1], -1).astype(jnp.bfloat16)


def feed_forward_kernel(
    n_ref, m_ref, w_ref, cg_ref, cv_ref, out_ref,
    all_ref, rim_ref, up_ref, down_ref, gate_ref, value_ref, p_ref, twin_buf, sum_buf, relay_buf,
    ring_buf, w_sem, ring_send, ring_recv, twin_send, twin_recv, rim_send, rim_recv, own_sem,
    pair_send, pair_recv, relay_send, relay_recv, back_send, back_recv,
):
    x, core = place_of()
    block = lax.axis_index("sp")
    rows, depth = n_ref.shape
    part = rows // 2
    tile = 2 * rows
    units = down_ref.shape[0]
    shards = w_ref.shape[0]
    deep = depth // shards
    right = (x + 1) % SIDE
    left = (x + 3) % SIDE
    across = (x + 2) % SIDE
    other = 2 * x + 1 - core
    halves = (slice(0, part), slice(part, rows))

    def weight_copies(k):
        at = slice(k * deep, (k + 1) * deep)
        return (
            pltpu.make_async_copy(
                w_ref.at[k, pl.ds(0, 2 * units)], up_ref.at[:, at], w_sem.at[0, k]
            ),
            pltpu.make_async_copy(
                w_ref.at[k, pl.ds(2 * units, units)], down_ref.at[:, at], w_sem.at[1, k]
            ),
        )

    for k in range(shards):
        for copy in weight_copies(k):
            copy.start()

    def spot(chip, half, of_core):
        return all_ref.at[2 * chip + of_core, pl.ds(half * part, part)]

    def ring(chip, half, to, lane):
        src = n_ref.at[pl.ds(half * part, part)] if chip is None else spot(chip, half, core)
        chip = x if chip is None else chip
        return remote_copy(
            src,
            spot(chip, half, core),
            ring_send.at[lane, half],
            ring_recv.at[chip, half],
            tp=2 * to + core,
        )

    def twin(chip, half):
        src = n_ref.at[pl.ds(half * part, part)] if chip is None else spot(chip, half, core)
        chip = x if chip is None else chip
        return remote_copy(
            src, spot(chip, half, core), twin_send.at[chip, half], twin_recv.at[chip, half], tp=other
        )

    def rim(to):
        return remote_copy(
            n_ref.at[pl.ds(rows - RIM, RIM)], rim_ref, rim_send.at[to], rim_recv, sp=block + 1, tp=to
        )

    last = (x == SIDE - 1) & (core == 1) & (block < SIDE * SIDE - 1)
    barrier = pltpu.get_barrier_semaphore()

    @pl.when(block > 0)
    def _():
        pl.semaphore_signal(
            barrier,
            inc=1,
            device_id={"sp": block - 1, "tp": 2 * SIDE - 1},
            device_id_type=pl.DeviceIdType.MESH,
        )

    meet(
        [{"tp": 2 * right + core}, {"tp": 2 * left + core}, {"tp": other}],
        jnp.where(last, 2 * SIDE, 0),
    )
    own = pltpu.make_async_copy(n_ref, all_ref.at[2 * x + core], own_sem)
    ring(None, 0, right, 0).start()
    ring(None, 1, left, 1).start()
    ring(None, 1, right, 0).start()
    ring(None, 0, left, 1).start()
    own.start()
    for half in range(2):
        twin(None, half).start()

    @pl.when(last)
    def _():
        for to in range(2 * SIDE):
            rim(to).start()

    def up(rows_in, which):
        w = up_ref[which * units : (which + 1) * units, :]
        return lax.dot_general(rows_in, w, NT, preferred_element_type=jnp.float32)

    def project_up(chip):
        rows_in = all_ref[pl.ds(2 * chip, 2)].reshape(tile, depth)
        for which, ref in enumerate((gate_ref, value_ref)):
            ref[pl.ds(pl.multiple_of(chip * tile + RIM, RIM), tile), :] = up(rows_in, which)

    def conv(ref, taps, chip):
        window = ref[pl.ds(pl.multiple_of(chip * tile, tile), tile + RIM), :]
        return (
            taps[0:1, :] * window[RIM - 2 : RIM - 2 + tile]
            + taps[1:2, :] * window[RIM - 1 : RIM - 1 + tile]
            + taps[2:3, :] * window[RIM : RIM + tile]
        )

    def project_down(chip):
        gate = conv(gate_ref, cg_ref, chip)
        value = conv(value_ref, cv_ref, chip)
        hidden = (gate / (1.0 + jnp.exp(-gate)) * value).astype(jnp.bfloat16)
        down = jnp.dot(hidden, down_ref[...], preferred_element_type=jnp.float32)
        p_ref[pl.ds(2 * chip, 2)] = down.astype(p_ref.dtype).reshape(2, rows, depth)

    def twin_arrived(chip):
        for half in range(2):
            arrived(spot(chip, half, 1 - core), twin_recv.at[chip, half])

    for k in range(shards):
        weight_copies(k)[0].wait()
    own.wait()
    twin_arrived(x)
    project_up(x)
    arrived(spot(left, 0, core), ring_recv.at[left, 0])
    ring(left, 0, right, 2).start()
    twin(left, 0).start()
    arrived(spot(right, 1, core), ring_recv.at[right, 1])
    ring(right, 1, left, 2).start()
    twin(right, 1).start()

    @pl.when(block > 0)
    def _():
        arrived(rim_ref, rim_recv)
        for which, ref in enumerate((gate_ref, value_ref)):
            ref[0:RIM, :] = up(rim_ref[...], which)

    @pl.when(block == 0)
    def _():
        for ref in (gate_ref, value_ref):
            ref[0:RIM, :] = jnp.zeros((RIM, units), jnp.float32)

    for chip, half in ((left, 1), (right, 0)):
        arrived(spot(chip, half, core), ring_recv.at[chip, half])
        twin(chip, half).start()
    twin_arrived(right)
    project_up(right)
    twin_arrived(left)
    project_up(left)
    for half in range(2):
        arrived(spot(across, half, core), ring_recv.at[across, half])
        twin(across, half).start()
    for k in range(shards):
        weight_copies(k)[1].wait()

    def pair(chip):
        return remote_copy(
            p_ref.at[2 * chip + 1 - core],
            twin_buf.at[chip],
            pair_send.at[chip],
            pair_recv.at[chip],
            tp=other,
        )

    def pair_sum(chip, half):
        mine = p_ref[2 * chip + core, halves[half], :].astype(jnp.float32)
        return mine + twin_buf[chip, halves[half], :].astype(jnp.float32)

    def relay(side):
        return remote_copy(
            sum_buf.at[0, halves[side]],
            relay_buf.at[side],
            relay_send.at[side],
            relay_recv.at[side],
            tp=2 * (right, left)[side] + core,
        )

    def back(side, half):
        return remote_copy(
            sum_buf.at[1 + side, halves[half]],
            ring_buf.at[side, halves[half]],
            back_send.at[side, half],
            back_recv.at[side, half],
            tp=2 * (right, left)[side] + core,
        )

    def direct(side):
        to = (right, left)[side]
        half = 1 - side
        arrived(twin_buf.at[to], pair_recv.at[to])
        sum_buf[1 + side, halves[half], :] = pair_sum(to, half).astype(jnp.bfloat16)
        back(side, half).start()

    project_down(right)
    pair(right).start()
    project_down(x)
    pair(x).start()
    direct(0)
    twin_arrived(across)
    project_up(across)
    project_down(across)
    pair(across).start()
    arrived(twin_buf.at[across], pair_recv.at[across])
    for side in range(2):
        sum_buf[0, halves[side], :] = pair_sum(across, side).astype(jnp.bfloat16)
        relay(side).start()
    project_down(left)
    pair(left).start()
    direct(1)
    arrived(twin_buf.at[x], pair_recv.at[x])
    for side in range(2):
        to = (right, left)[side]
        arrived(relay_buf.at[side], relay_recv.at[side])
        total = pair_sum(to, side) + relay_buf[side].astype(jnp.float32)
        sum_buf[1 + side, halves[side], :] = total.astype(jnp.bfloat16)
        back(side, side).start()
    for half in range(2):
        total = m_ref[halves[half], :].astype(jnp.float32) + pair_sum(x, half)
        for side in (1 - half, half):
            arrived(ring_buf.at[side, halves[half]], back_recv.at[side, half])
            total = total + ring_buf[side, halves[half], :].astype(jnp.float32)
        out_ref[halves[half], :] = total.astype(out_ref.dtype)

    for half in range(2):
        ring(None, half, right, 0).wait_send()
        ring(None, half, left, 1).wait_send()
        twin(None, half).wait_send()
        for chip in (left, right, across):
            twin(chip, half).wait_send()
    ring(left, 0, right, 2).wait_send()
    ring(right, 1, left, 2).wait_send()

    @pl.when(last)
    def _():
        for to in range(2 * SIDE):
            rim(to).wait_send()

    for chip in range(SIDE):
        pair(chip).wait_send()
    for side in range(2):
        relay(side).wait_send()
        for half in range(2):
            back(side, half).wait_send()


def feed_forward(normed, middle, whole, conv_gate, conv_value):
    rows, depth = normed.shape
    units = conv_gate.shape[1]
    total = 2 * SIDE * rows
    vmem = pl.BlockSpec(memory_space=pltpu.VMEM)
    dma = pltpu.SemaphoreType.DMA
    bf16 = jnp.bfloat16
    return pl.pallas_call(
        feed_forward_kernel,
        out_shape=jax.ShapeDtypeStruct((rows, depth), bf16),
        in_specs=[vmem, vmem, pl.BlockSpec(memory_space=pl.ANY), vmem, vmem],
        out_specs=vmem,
        scratch_shapes=[
            pltpu.VMEM((2 * SIDE, rows, depth), bf16),
            pltpu.VMEM((RIM, depth), bf16),
            pltpu.VMEM((2 * units, depth), bf16),
            pltpu.VMEM((units, depth), bf16),
            pltpu.VMEM((RIM + total, units), jnp.float32),
            pltpu.VMEM((RIM + total, units), jnp.float32),
            pltpu.VMEM((2 * SIDE, rows, depth), bf16),
            pltpu.VMEM((SIDE, rows, depth), bf16),
            pltpu.VMEM((3, rows, depth), bf16),
            pltpu.VMEM((2, rows // 2, depth), bf16),
            pltpu.VMEM((2, rows, depth), bf16),
            dma((2, whole.shape[0])),
            dma((3, 2)), dma((SIDE, 2)), dma((SIDE, 2)), dma((SIDE, 2)), dma((2 * SIDE,)), dma(()), dma(()),
            dma((SIDE,)), dma((SIDE,)), dma((2,)), dma((2,)), dma((2, 2)), dma((2, 2)),
        ],
        compiler_params=pltpu.CompilerParams(
            has_side_effects=True, collective_id=1, vmem_limit_bytes=VMEM
        ),
        cost_estimate=pl.CostEstimate(
            flops=9 * 10**9, bytes_accessed=12 * 2**20, transcendentals=0
        ),
        name="feed_forward",
    )(normed, middle, whole, conv_gate, conv_value)


def local(
    queries,
    keys,
    values,
    stick_bias,
    residual,
    out_weight,
    norm_gain,
    gate_weight,
    value_weight,
    down_weight,
    conv_gate,
    conv_value,
):
    rows_here = queries.shape[0]
    model_width = residual.shape[1]
    bias_rows = stick_bias.reshape(rows_here // CHUNK, CHUNK)
    bias_rows = jnp.pad(bias_rows, ((0, PAD - bias_rows.shape[0]), (0, 0)))
    weights = jnp.concatenate([gate_weight.T, value_weight.T, down_weight.T], axis=0)
    parts, logs, whole = attend(
        queries, keys, values, bias_rows, weights, lax.axis_size("tp")
    )
    row_heads = combine(parts, logs)
    projected = jnp.dot(row_heads, out_weight, preferred_element_type=jnp.float32)
    middle = (residual.astype(jnp.float32) + projected).astype(jnp.bfloat16)
    middle_f = middle.astype(jnp.float32)
    normed = (
        middle_f
        * lax.rsqrt(jnp.mean(middle_f * middle_f, axis=-1, keepdims=True) + EPS)
        * norm_gain
    ).astype(jnp.bfloat16)
    return feed_forward(normed, middle, whole, conv_gate, conv_value)


def solution(mesh):
    in_specs = (
        P("sp", "tp"),
        P("sp", "tp"),
        P("sp", "tp"),
        P("sp", "tp"),
        P(("sp", "tp"), None),
        P(),
        P(),
        P("sp", "tp"),
        P("sp", "tp"),
        P("sp", "tp"),
        P(None, "tp"),
        P(None, "tp"),
    )
    out_specs = P(("sp", "tp"), None)
    return jax.shard_map(local, mesh=mesh, in_specs=in_specs, out_specs=out_specs, check_vma=False)
```

```python
import jax
import jax.numpy as jnp
from jax import lax
from jax.experimental import pallas as pl
from jax.experimental.pallas import tpu as pltpu
from jax.sharding import PartitionSpec as P

EPS = 1e-06
LOG2E = 1.4426950408889634
NT = (((1,), (1,)), ((), ()))
CHUNK = 256
PAD = 16
SIDE = 4
RIM = 16
VMEM = 67_000_000
ATTEND = 28
STAGES = (
    (0, 0, 3), (1, 0, 4), (2, 0, 5), (3, 0, 6), (4, 0, 7), (6, 0, 8), (11, 1, 0), (11, 1, 1),
)


def tri_matrix():
    rows = lax.broadcasted_iota(jnp.int32, (CHUNK, CHUNK), 0)
    cols = lax.broadcasted_iota(jnp.int32, (CHUNK, CHUNK), 1)
    return (rows > cols).astype(jnp.bfloat16), rows > cols


def visit_chunk(q, k, v, bias, tri, gone, acc, mask=None):
    scale = 128 ** (-0.5) * LOG2E
    s = lax.dot_general(q, k, NT, preferred_element_type=jnp.float32) * scale + bias
    if mask is not None:
        s = jnp.where(mask, s, -1e30)
    soft = jnp.maximum(jnp.log(1.0 + jnp.exp2(jnp.minimum(s, 126.0))) * LOG2E, s)
    behind = jnp.dot(soft.astype(jnp.bfloat16), tri, preferred_element_type=jnp.float32)
    stick = jnp.exp2((s - soft) - (behind + gone)).astype(jnp.bfloat16)
    acc = acc + jnp.dot(stick, v, preferred_element_type=jnp.float32)
    gone = gone + (behind[:, 0:1] + soft[:, 0:1])
    return gone, acc


def position():
    me = lax.axis_index("sp")
    return me, me // SIDE, me % SIDE


def owners_of(y):
    core = lax.axis_index("tp") % 2
    return 2 * ((y + core) % SIDE), 2 * ((y + core + 2) % SIDE) + 1


def place_of():
    me = lax.axis_index("tp")
    return me // 2, me % 2


def remote_copy(src, dst, send_sem, recv_sem, **where):
    return pltpu.make_async_remote_copy(
        src_ref=src,
        dst_ref=dst,
        send_sem=send_sem,
        recv_sem=recv_sem,
        device_id=where,
        device_id_type=pl.DeviceIdType.MESH,
    )


def arrived(dst, sem):
    pltpu.make_async_copy(dst, dst, sem).wait()


def meet(peers, extra=0):
    barrier = pltpu.get_barrier_semaphore()
    for where in peers:
        pl.semaphore_signal(barrier, inc=1, device_id=where, device_id_type=pl.DeviceIdType.MESH)
    pl.semaphore_wait(barrier, len(peers) + extra)


def attend_part(
    q_ref, k_ref, v_ref, b_ref, w_ref, os_ref, gs_ref, whole_ref,
    q_all, k_all, v_all, b_all, o_buf, g_buf, acc_ref, gone_ref, block_out, block_gone,
    kv_send, kv_recv, kv_own, bias_send, bias_recv, bias_own, q_send, q_recv, q_own, z_send, z_recv,
    w1_send, w1_relay, w2_send, w2_relay, w_recv, o_send, o_recv,
):
    me, z, y = position()
    x, core = place_of()
    head = lax.axis_index("tp")
    rows, width = k_ref.shape
    quarter = rows // SIDE
    share = quarter // 2
    chunks = rows // CHUNK
    right = (y + 1) % SIDE
    left = (y + 3) % SIDE
    across = (y + 2) % SIDE
    row = z * SIDE
    owners = owners_of(y)
    tri, _ = tri_matrix()

    barrier = pltpu.get_barrier_semaphore()

    def greet(group, carry):
        for source in range(os_ref.shape[0]):
            of = (x - source % 2 - 2 * core + 2 * SIDE) % SIDE
            pl.semaphore_signal(
                barrier,
                inc=1,
                device_id={"sp": group * SIDE + of, "tp": source},
                device_id_type=pl.DeviceIdType.MESH,
            )
        return carry

    lax.fori_loop(0, z + 1, greet, 0)

    @pl.when(me > 0)
    def _():
        pl.semaphore_signal(
            barrier,
            inc=1,
            device_id={"sp": me - 1, "tp": 2 * SIDE - 1},
            device_id_type=pl.DeviceIdType.MESH,
        )

    meet(
        [{"sp": row + (y + d) % SIDE} for d in (1, 2, 3)]
        + [{"sp": (z + d) % SIDE * SIDE + y} for d in (1, 2, 3)]
        + [{"tp": 2 * ((x + d) % SIDE) + core} for d in (1, 3)]
        + [{"tp": 2 * x + 1 - core}],
        2 * (SIDE * SIDE - row)
        + jnp.where((head == 2 * SIDE - 1) & (me < SIDE * SIDE - 1), 2 * SIDE, 0),
    )

    def hop(part, src_slot, to, lane):
        src = (k_ref, v_ref)[part] if src_slot is None else (k_all, v_all)[part].at[src_slot]
        slot = y if src_slot is None else src_slot
        return remote_copy(
            src,
            (k_all, v_all)[part].at[slot],
            kv_send.at[part, lane],
            kv_recv.at[part, slot],
            sp=row + to,
        )

    def kv_mine(part):
        return pltpu.make_async_copy(
            (k_ref, v_ref)[part], (k_all, v_all)[part].at[y], kv_own.at[part]
        )

    def bias_hop(d):
        return remote_copy(
            b_ref, b_all.at[y], bias_send.at[d], bias_recv.at[y], sp=row + (y + d) % SIDE
        )

    def q_source(of, half):
        return q_ref.at[pl.ds(pl.multiple_of(owners_of(of)[half] * share, share), share)]

    def q_mine(half):
        return pltpu.make_async_copy(
            q_source(y, half), q_all.at[me, pl.ds(half * share, share)], q_own.at[half]
        )

    def q_piece(d, half):
        of = (y + d) % SIDE
        return remote_copy(
            q_source(of, half),
            q_all.at[me, pl.ds(half * share, share)],
            q_send.at[d, half],
            q_recv.at[y, half],
            sp=row + of,
        )

    def q_down(dz):
        ours = q_all.at[pl.ds(pl.multiple_of(row, SIDE), SIDE)]
        return remote_copy(ours, ours, z_send.at[dz], z_recv.at[z], sp=row - dz * SIDE + y)

    third = w_ref.shape[0] // 3
    starts = (0, 2 * third)
    bulks = (third, third // 2)
    steps = (0, 3, 1, 2)

    def w_axes(part):
        return (y, z) if part == 0 else (z, y)

    def w_index(part, c1, c2):
        return c2 * SIDE + c1 if part == 0 else c1 * SIDE + c2

    def w_rows(batch, part, half):
        piece = bulks[batch] // 2
        return pl.ds(starts[batch] + (2 * part + half) * piece, piece)

    def w_copy(batch, part, half, c1, c2, own, to1, to2, send):
        slot = w_index(part, c1, c2)
        spot = whole_ref.at[slot, w_rows(batch, part, half)]
        src = w_ref.at[w_rows(batch, part, half)] if own else spot
        return remote_copy(
            src, spot, send, w_recv.at[batch, part, slot, half], sp=w_index(part, to1, to2)
        )

    def w_first(batch, part, way, half):
        c1, c2 = w_axes(part)
        to = (c1 + (1, 3)[way]) % SIDE
        return w_copy(batch, part, half, c1, c2, True, to, c2, w1_send.at[batch, part, way, half])

    def w_first_relay(batch, part, way):
        c1, c2 = w_axes(part)
        source = (c1 + (3, 1)[way]) % SIDE
        to = (c1 + (1, 3)[way]) % SIDE
        return w_copy(batch, part, way, source, c2, False, to, c2, w1_relay.at[batch, part, way])

    def w_second(batch, part, k, way, half):
        c1, c2 = w_axes(part)
        to = (c2 + (1, 3)[way]) % SIDE
        source = (c1 + steps[k]) % SIDE
        return w_copy(batch, part, half, source, c2, k == 0, c1, to, w2_send.at[batch, part, k, way, half])

    def w_second_relay(batch, part, k, way):
        c1, c2 = w_axes(part)
        source = (c2 + (3, 1)[way]) % SIDE
        to = (c2 + (1, 3)[way]) % SIDE
        return w_copy(
            batch, part, way, (c1 + steps[k]) % SIDE, source, False, c1, to, w2_relay.at[batch, part, k, way]
        )

    def w_take(batch, part, half, c1, c2):
        slot = w_index(part, c1, c2)
        arrived(whole_ref.at[slot, w_rows(batch, part, half)], w_recv.at[batch, part, slot, half])

    def w_near(part):
        c1, c2 = w_axes(part)
        return (c1 + 3) % SIDE, (c1 + 1) % SIDE, (c1 + 2) % SIDE, c2

    def w_own(batch, first_part):
        for half in range(2):
            for way in range(2):
                of = (half + way) % 2
                w_first(batch, first_part, way, of).start()
                w_second(batch, 1 - first_part, 0, way, of).start()

    def w_stage(batch, stage):
        if stage == 0:
            w_own(batch, 0)
        elif stage == 1:
            w_own(batch, 1)
        elif stage == 2:
            for way in range(2):
                for part in (1, 0):
                    near = w_near(part)
                    w_take(batch, part, way, near[way], near[3])
                    w_first_relay(batch, part, way).start()
        elif stage == 3:
            for part in (1, 0):
                near = w_near(part)
                for way in range(2):
                    w_take(batch, part, 1 - way, near[way], near[3])
            for half in range(2):
                for k in (1, 2):
                    for way in range(2):
                        for part in (1, 0):
                            w_second(batch, part, k, way, (half + way) % 2).start()
        elif stage == 4:
            for part in (1, 0):
                near = w_near(part)
                for half in range(2):
                    w_take(batch, part, half, near[2], near[3])
            for half in range(2):
                for way in range(2):
                    for part in (1, 0):
                        w_second(batch, part, 3, way, (half + way) % 2).start()
        elif stage < 9:
            k = stage - 5
            for way in range(2):
                for part in (1, 0):
                    c1, c2 = w_axes(part)
                    w_take(batch, part, way, (c1 + steps[k]) % SIDE, (c2 + (3, 1)[way]) % SIDE)
                    w_second_relay(batch, part, k, way).start()
        else:
            for part in range(2):
                c1, c2 = w_axes(part)
                for k in range(SIDE):
                    source = (c1 + steps[k]) % SIDE
                    w_take(batch, part, 1, source, (c2 + 3) % SIDE)
                    w_take(batch, part, 0, source, (c2 + 1) % SIDE)
                    for half in range(2):
                        w_take(batch, part, half, source, (c2 + 2) % SIDE)

    def w_sent():
        for batch in range(2):
            for part in range(2):
                for way in range(2):
                    w_first_relay(batch, part, way).wait_send()
                    for half in range(2):
                        w_first(batch, part, way, half).wait_send()
                    for k in range(SIDE):
                        w_second_relay(batch, part, k, way).wait_send()
                        for half in range(2):
                            w_second(batch, part, k, way, half).wait_send()

    def out_pieces(block, half):
        src = o_buf.at[block, pl.ds(half * share, share)]
        return ((src, os_ref), (g_buf.at[block, half], gs_ref))

    def out_remote(block, half, part):
        src, dst = out_pieces(block, half)[part]
        return remote_copy(
            src,
            dst.at[head, z],
            o_send.at[part, block, half],
            o_recv.at[part, head, z],
            sp=block,
            tp=owners[half],
        )

    def out_local(block, half, part):
        src, dst = out_pieces(block, half)[part]
        return pltpu.make_async_copy(src, dst.at[head, z], o_recv.at[part, head, z])

    def for_outs(group, act, act_local):
        for m in range(SIDE):
            block = group * SIDE + m
            for half in range(2):
                mine = (block == me) & (owners[half] == head)
                if act_local is not None:

                    @pl.when(mine)
                    def _():
                        for part in range(2):
                            act_local(out_local(block, half, part))

                @pl.when(jnp.logical_not(mine))
                def _():
                    for part in range(2):
                        act(out_remote(block, half, part))

    def finish(group):
        acc = acc_ref[...]
        gone = gone_ref[...]
        for m in range(SIDE):
            here = slice(m * quarter, (m + 1) * quarter)
            o_buf[group * SIDE + m] = acc[here].astype(o_buf.dtype)
            turned = gone[here].T
            for half in range(2):
                g_buf[group * SIDE + m, half] = turned[0:8, half * 128 : (half + 1) * 128]
        for_outs(group, lambda copy: copy.start(), lambda copy: copy.start())

    w_stage(0, 1)
    for half in range(2):
        q_mine(half).start()
    for d in (2, 1, 3):
        for half in range(2):
            q_piece(d, half).start()
        bias_hop(d).start()
    hop(0, None, right, 0).start()
    hop(1, None, left, 0).start()
    hop(1, None, right, 1).start()
    hop(0, None, left, 1).start()
    for part in range(2):
        kv_mine(part).start()
    bias_mine = pltpu.make_async_copy(b_ref, b_all.at[y], bias_own)
    bias_mine.start()

    first, second = (owner * share for owner in owners)
    at_row = lax.broadcasted_iota(jnp.int32, (rows, CHUNK), 0)
    col = lax.broadcasted_iota(jnp.int32, (rows, CHUNK), 1)
    inside = at_row % quarter
    place = (
        at_row // quarter * rows
        + inside
        + jnp.where(inside < share, first, second - share)
        - col
    )

    def diagonal(i, carry):
        j = (y + jnp.where(i == 0, 0, jnp.where(i == 1, 3, i - 1))) % SIDE

        @pl.when(i == 0)
        def _():
            for half in range(2):
                q_mine(half).wait()
                for d in (1, 2, 3):
                    slot = (y + d) % SIDE
                    arrived(q_all.at[row + slot, pl.ds(half * share, share)], q_recv.at[slot, half])
            for dz in (2, 3, 1):

                @pl.when(z >= dz)
                def _():
                    q_down(dz).start()

            for part in range(2):
                kv_mine(part).wait()
            bias_mine.wait()

        @pl.when(i == 1)
        def _():
            arrived(k_all.at[left], kv_recv.at[0, left])
            hop(0, left, right, 2).start()
            arrived(v_all.at[right], kv_recv.at[1, right])
            hop(1, right, left, 2).start()
            w_stage(0, 0)
            arrived(v_all.at[left], kv_recv.at[1, left])
            arrived(b_all.at[left], bias_recv.at[left])

        @pl.when(i == 2)
        def _():
            arrived(k_all.at[right], kv_recv.at[0, right])
            arrived(b_all.at[right], bias_recv.at[right])

        @pl.when(i == 3)
        def _():
            arrived(k_all.at[across], kv_recv.at[0, across])
            arrived(v_all.at[across], kv_recv.at[1, across])
            arrived(b_all.at[across], bias_recv.at[across])

        q = q_all[pl.ds(row, SIDE)].reshape(rows, width)
        bias = b_all[j].astype(jnp.float32) * LOG2E
        gone = jnp.zeros((rows, 1), jnp.float32)
        acc = jnp.zeros((rows, width), jnp.float32)
        for c in range(chunks - 1, -1, -1):
            at = slice(c * CHUNK, (c + 1) * CHUNK)
            mask = place > j * rows + c * CHUNK
            gone, acc = visit_chunk(
                q, k_all[j, at, :], v_all[j, at, :], bias[c : c + 1, :], tri, gone, acc, mask
            )
        block_out[j] = acc
        block_gone[j] = jnp.broadcast_to(gone, (rows, 128))
        return carry

    lax.fori_loop(0, SIDE, diagonal, 0)
    gone = block_gone[SIDE - 1]
    acc = block_out[SIDE - 1]
    for j in range(SIDE - 2, -1, -1):
        acc = acc + jnp.exp2(-gone) * block_out[j]
        gone = gone + block_gone[j]
    acc_ref[...] = acc
    gone_ref[...] = gone
    finish(z)
    w_stage(0, 2)
    for other in range(1, SIDE):

        @pl.when(z < other)
        def _():
            arrived(q_all.at[pl.ds(other * SIDE, SIDE)], z_recv.at[other])

    def step(s, carry):
        group = z + 1 + s // SIDE
        j = SIDE - 1 - s % SIDE

        @pl.when(group < SIDE)
        def _():
            @pl.when(j == SIDE - 1)
            def _():
                acc_ref[...] = jnp.zeros_like(acc_ref)
                gone_ref[...] = jnp.zeros_like(gone_ref)

            q = q_all[pl.ds(group * SIDE, SIDE)].reshape(rows, width)
            bias = b_all[j].astype(jnp.float32) * LOG2E
            gone = gone_ref[:, 0:1]
            acc = acc_ref[...]
            for c in range(chunks - 1, -1, -1):
                at = slice(c * CHUNK, (c + 1) * CHUNK)
                gone, acc = visit_chunk(
                    q, k_all[j, at, :], v_all[j, at, :], bias[c : c + 1, :], tri, gone, acc
                )
            acc_ref[...] = acc
            gone_ref[...] = jnp.broadcast_to(gone, (rows, 128))

            @pl.when(j == 0)
            def _():
                finish(group)

        for after, batch, stage in STAGES:

            @pl.when(s == after)
            def _():
                w_stage(batch, stage)

        return carry

    lax.fori_loop(0, (SIDE - 1) * SIDE, step, 0)

    def take(group, carry):
        for h in range(os_ref.shape[0]):
            for part in range(2):
                arrived((os_ref, gs_ref)[part].at[h, group], o_recv.at[part, h, group])
        return carry

    lax.fori_loop(0, z + 1, take, 0)
    def up_weights():
        w_stage(0, 9)

    def down_weights(stage):
        w_stage(1, stage)

    def all_sent():
        def sent(group, carry):
            for_outs(group, lambda copy: copy.wait_send(), None)
            return carry

        lax.fori_loop(z, SIDE, sent, 0)
        w_sent()
        hop(0, None, right, 0).wait_send()
        hop(1, None, left, 0).wait_send()
        hop(1, None, right, 1).wait_send()
        hop(0, None, left, 1).wait_send()
        hop(0, left, right, 2).wait_send()
        hop(1, right, left, 2).wait_send()
        for d in (1, 2, 3):
            bias_hop(d).wait_send()
            for half in range(2):
                q_piece(d, half).wait_send()
        for dz in (1, 2, 3):

            @pl.when(z >= dz)
            def _():
                q_down(dz).wait_send()

    return up_weights, down_weights, all_sent


def feed_forward_part(
    up_weights, down_weights, n_ref, m_ref, mine_ref, w_ref, cg_ref, cv_ref, out_ref,
    all_ref, rim_ref, up_ref, down_ref, gate_ref, value_ref, p_ref, twin_buf, sum_buf, relay_buf,
    ring_buf, w_sem, ring_send, ring_recv, twin_send, twin_recv, rim_send, rim_recv, own_sem,
    pair_send, pair_recv, relay_send, relay_recv, back_send, back_recv,
):
    x, core = place_of()
    block = lax.axis_index("sp")
    rows, depth = n_ref.shape
    part = rows // 2
    tile = 2 * rows
    units = down_ref.shape[0]
    shards = w_ref.shape[0]
    deep = depth // shards
    right = (x + 1) % SIDE
    left = (x + 3) % SIDE
    across = (x + 2) % SIDE
    other = 2 * x + 1 - core
    halves = (slice(0, part), slice(part, rows))

    def up_copy(k, src):
        at = slice(k * deep, (k + 1) * deep)
        return pltpu.make_async_copy(src.at[pl.ds(0, 2 * units)], up_ref.at[:, at], w_sem.at[0, k])

    def down_copy(k, src):
        at = slice(k * deep, (k + 1) * deep)
        return pltpu.make_async_copy(
            src.at[pl.ds(2 * units, units)], down_ref.at[:, at], w_sem.at[1, k]
        )

    def load(copy):
        for k in range(shards):

            @pl.when(block == k)
            def _():
                copy(k, mine_ref).start()

            @pl.when(block != k)
            def _():
                copy(k, w_ref.at[k]).start()

    def spot(chip, half, of_core):
        return all_ref.at[2 * chip + of_core, pl.ds(half * part, part)]

    def ring(chip, half, to, lane):
        src = n_ref.at[pl.ds(half * part, part)] if chip is None else spot(chip, half, core)
        chip = x if chip is None else chip
        return remote_copy(
            src,
            spot(chip, half, core),
            ring_send.at[lane, half],
            ring_recv.at[chip, half],
            tp=2 * to + core,
        )

    def twin(chip, half):
        src = n_ref.at[pl.ds(half * part, part)] if chip is None else spot(chip, half, core)
        chip = x if chip is None else chip
        return remote_copy(
            src, spot(chip, half, core), twin_send.at[chip, half], twin_recv.at[chip, half], tp=other
        )

    def rim(to):
        return remote_copy(
            n_ref.at[pl.ds(rows - RIM, RIM)], rim_ref, rim_send.at[to], rim_recv, sp=block + 1, tp=to
        )

    last = (x == SIDE - 1) & (core == 1) & (block < SIDE * SIDE - 1)
    own = pltpu.make_async_copy(n_ref, all_ref.at[2 * x + core], own_sem)
    ring(None, 0, right, 0).start()
    ring(None, 1, left, 1).start()
    ring(None, 1, right, 0).start()
    ring(None, 0, left, 1).start()
    own.start()
    for half in range(2):
        twin(None, half).start()

    @pl.when(last)
    def _():
        for to in range(2 * SIDE):
            rim(to).start()

    def up(rows_in, which):
        w = up_ref[which * units : (which + 1) * units, :]
        return lax.dot_general(rows_in, w, NT, preferred_element_type=jnp.float32)

    def project_up(chip):
        rows_in = all_ref[pl.ds(2 * chip, 2)].reshape(tile, depth)
        for which, ref in enumerate((gate_ref, value_ref)):
            ref[pl.ds(pl.multiple_of(chip * tile + RIM, RIM), tile), :] = up(rows_in, which)

    def conv(ref, taps, chip):
        window = ref[pl.ds(pl.multiple_of(chip * tile, tile), tile + RIM), :]
        return (
            taps[0:1, :] * window[RIM - 2 : RIM - 2 + tile]
            + taps[1:2, :] * window[RIM - 1 : RIM - 1 + tile]
            + taps[2:3, :] * window[RIM : RIM + tile]
        )

    def project_down(chip):
        gate = conv(gate_ref, cg_ref, chip)
        value = conv(value_ref, cv_ref, chip)
        hidden = (gate / (1.0 + jnp.exp(-gate)) * value).astype(jnp.bfloat16)
        down = jnp.dot(hidden, down_ref[...], preferred_element_type=jnp.float32)
        p_ref[pl.ds(2 * chip, 2)] = down.astype(p_ref.dtype).reshape(2, rows, depth)

    def twin_arrived(chip):
        for half in range(2):
            arrived(spot(chip, half, 1 - core), twin_recv.at[chip, half])

    up_weights()
    load(up_copy)
    down_weights(2)
    for k in range(shards):
        up_copy(k, mine_ref).wait()
    own.wait()
    twin_arrived(x)
    project_up(x)
    down_weights(3)
    arrived(spot(left, 0, core), ring_recv.at[left, 0])
    ring(left, 0, right, 2).start()
    twin(left, 0).start()
    arrived(spot(right, 1, core), ring_recv.at[right, 1])
    ring(right, 1, left, 2).start()
    twin(right, 1).start()

    down_weights(4)

    @pl.when(block > 0)
    def _():
        arrived(rim_ref, rim_recv)
        for which, ref in enumerate((gate_ref, value_ref)):
            ref[0:RIM, :] = up(rim_ref[...], which)

    @pl.when(block == 0)
    def _():
        for ref in (gate_ref, value_ref):
            ref[0:RIM, :] = jnp.zeros((RIM, units), jnp.float32)

    for chip, half in ((left, 1), (right, 0)):
        arrived(spot(chip, half, core), ring_recv.at[chip, half])
        twin(chip, half).start()
    down_weights(5)
    down_weights(6)
    twin_arrived(right)
    project_up(right)
    down_weights(7)
    down_weights(8)
    twin_arrived(left)
    project_up(left)
    down_weights(9)
    load(down_copy)
    for half in range(2):
        arrived(spot(across, half, core), ring_recv.at[across, half])
        twin(across, half).start()
    for k in range(shards):
        down_copy(k, mine_ref).wait()

    def pair(chip):
        return remote_copy(
            p_ref.at[2 * chip + 1 - core],
            twin_buf.at[chip],
            pair_send.at[chip],
            pair_recv.at[chip],
            tp=other,
        )

    def pair_sum(chip, half):
        mine = p_ref[2 * chip + core, halves[half], :].astype(jnp.float32)
        return mine + twin_buf[chip, halves[half], :].astype(jnp.float32)

    def relay(side):
        return remote_copy(
            sum_buf.at[0, halves[side]],
            relay_buf.at[side],
            relay_send.at[side],
            relay_recv.at[side],
            tp=2 * (right, left)[side] + core,
        )

    def back(side, half):
        return remote_copy(
            sum_buf.at[1 + side, halves[half]],
            ring_buf.at[side, halves[half]],
            back_send.at[side, half],
            back_recv.at[side, half],
            tp=2 * (right, left)[side] + core,
        )

    def direct(side):
        to = (right, left)[side]
        half = 1 - side
        arrived(twin_buf.at[to], pair_recv.at[to])
        sum_buf[1 + side, halves[half], :] = pair_sum(to, half).astype(jnp.bfloat16)
        back(side, half).start()

    project_down(right)
    pair(right).start()
    project_down(x)
    pair(x).start()
    direct(0)
    twin_arrived(across)
    project_up(across)
    project_down(across)
    pair(across).start()
    arrived(twin_buf.at[across], pair_recv.at[across])
    for side in range(2):
        sum_buf[0, halves[side], :] = pair_sum(across, side).astype(jnp.bfloat16)
        relay(side).start()
    project_down(left)
    pair(left).start()
    direct(1)
    arrived(twin_buf.at[x], pair_recv.at[x])
    for side in range(2):
        to = (right, left)[side]
        arrived(relay_buf.at[side], relay_recv.at[side])
        total = pair_sum(to, side) + relay_buf[side].astype(jnp.float32)
        sum_buf[1 + side, halves[side], :] = total.astype(jnp.bfloat16)
        back(side, side).start()
    for half in range(2):
        total = m_ref[halves[half], :].astype(jnp.float32) + pair_sum(x, half)
        for side in (1 - half, half):
            arrived(ring_buf.at[side, halves[half]], back_recv.at[side, half])
            total = total + ring_buf[side, halves[half], :].astype(jnp.float32)
        out_ref[halves[half], :] = total.astype(out_ref.dtype)

    for half in range(2):
        ring(None, half, right, 0).wait_send()
        ring(None, half, left, 1).wait_send()
        twin(None, half).wait_send()
        for chip in (left, right, across):
            twin(chip, half).wait_send()
    ring(left, 0, right, 2).wait_send()
    ring(right, 1, left, 2).wait_send()

    @pl.when(last)
    def _():
        for to in range(2 * SIDE):
            rim(to).wait_send()

    for chip in range(SIDE):
        pair(chip).wait_send()
    for side in range(2):
        relay(side).wait_send()
        for half in range(2):
            back(side, half).wait_send()


def middle_part(os_ref, gs_ref, res_ref, ow_ref, gain_ref, m_ref, n_ref):
    z = position()[1]
    heads, groups, rows, width = os_ref.shape
    outs = [jnp.zeros((rows, width), jnp.float32) for _ in range(heads)]
    later = jnp.zeros((rows, 128), jnp.float32)
    for group in range(groups - 1, -1, -1):
        valid = group <= z
        weight = jnp.exp2(-later)
        for h in range(heads):
            term = jnp.where(valid, os_ref[h, group].astype(jnp.float32), 0.0)
            outs[h] = outs[h] + term * weight[:, h : h + 1]
        if group:
            left = jnp.concatenate([gs_ref[h, group, 0:1, :] for h in range(heads)], axis=0)
            left = jnp.where(valid, left, 0.0)
            later = later + jnp.concatenate([left] * (128 // heads), axis=0).T
    attended = jnp.concatenate(outs, axis=1).astype(jnp.bfloat16)
    projected = jnp.dot(attended, ow_ref[...], preferred_element_type=jnp.float32)
    middle = (res_ref[...].astype(jnp.float32) + projected).astype(jnp.bfloat16)
    m_ref[...] = middle
    wide = middle.astype(jnp.float32)
    scale = lax.rsqrt(jnp.mean(wide * wide, axis=-1, keepdims=True) + EPS)
    n_ref[...] = (wide * scale * gain_ref[...]).astype(jnp.bfloat16)


def layer_kernel(*refs):
    q, k, v, b, w, res, ow, gain, cg, cv, out, whole = refs[:12]
    os_ref, gs_ref, ow_ref, m_ref, n_ref, ow_sem = refs[12:18]
    attend_refs = refs[18 : 18 + ATTEND]
    ff_refs = refs[18 + ATTEND :]
    ow_copy = pltpu.make_async_copy(ow, ow_ref, ow_sem)
    ow_copy.start()
    up_weights, down_weights, all_sent = attend_part(q, k, v, b, w, os_ref, gs_ref, whole, *attend_refs)
    ow_copy.wait()
    middle_part(os_ref, gs_ref, res, ow_ref, gain, m_ref, n_ref)
    feed_forward_part(up_weights, down_weights, n_ref, m_ref, w, whole, cg, cv, out, *ff_refs)
    all_sent()


def layer(queries, keys, values, bias_rows, weights, residual, out_weight, gain, conv_gate, conv_value):
    rows, width = queries.shape
    share, depth = residual.shape
    units = conv_gate.shape[1]
    heads = lax.axis_size("tp")
    count = SIDE * SIDE
    quarter = rows // SIDE
    anywhere = pl.BlockSpec(memory_space=pl.ANY)
    vmem = pl.BlockSpec(memory_space=pltpu.VMEM)
    dma = pltpu.SemaphoreType.DMA
    bf16 = jnp.bfloat16
    f32 = jnp.float32
    attend_scratch = [
        pltpu.VMEM((count, quarter, width), bf16),
        pltpu.VMEM((SIDE, rows, width), bf16),
        pltpu.VMEM((SIDE, rows, width), bf16),
        pltpu.VMEM((SIDE,) + bias_rows.shape, bf16),
        pltpu.VMEM((count, quarter, width), bf16),
        pltpu.VMEM((count, 2, 8, 128), f32),
        pltpu.VMEM((rows, width), f32),
        pltpu.VMEM((rows, 128), f32),
        pltpu.VMEM((SIDE, rows, width), f32),
        pltpu.VMEM((SIDE, rows, 128), f32),
        dma((2, 3)), dma((2, SIDE)), dma((2,)), dma((SIDE,)), dma((SIDE,)), dma(()),
        dma((SIDE, 2)), dma((SIDE, 2)), dma((2,)), dma((SIDE,)), dma((SIDE,)),
        dma((2, 2, 2, 2)), dma((2, 2, 2)), dma((2, 2, SIDE, 2, 2)), dma((2, 2, SIDE, 2)),
        dma((2, 2, count, 2)), dma((2, count, 2)), dma((2, heads, SIDE)),
    ]
    ff_scratch = [
        pltpu.VMEM((2 * SIDE, share, depth), bf16),
        pltpu.VMEM((RIM, depth), bf16),
        pltpu.VMEM((2 * units, depth), bf16),
        pltpu.VMEM((units, depth), bf16),
        pltpu.VMEM((RIM + rows, units), f32),
        pltpu.VMEM((RIM + rows, units), f32),
        pltpu.VMEM((2 * SIDE, share, depth), bf16),
        pltpu.VMEM((SIDE, share, depth), bf16),
        pltpu.VMEM((3, share, depth), bf16),
        pltpu.VMEM((2, share // 2, depth), bf16),
        pltpu.VMEM((2, share, depth), bf16),
        dma((2, count)),
        dma((3, 2)), dma((SIDE, 2)), dma((SIDE, 2)), dma((SIDE, 2)), dma((2 * SIDE,)), dma(()), dma(()),
        dma((SIDE,)), dma((SIDE,)), dma((2,)), dma((2,)), dma((2, 2)), dma((2, 2)),
    ]
    assert len(attend_scratch) == ATTEND
    return pl.pallas_call(
        layer_kernel,
        out_shape=(
            jax.ShapeDtypeStruct((share, depth), bf16),
            jax.ShapeDtypeStruct((count,) + weights.shape, bf16),
        ),
        in_specs=[anywhere, anywhere, anywhere, vmem, anywhere, vmem, anywhere, vmem, vmem, vmem],
        out_specs=[vmem, anywhere],
        scratch_shapes=[
            pltpu.VMEM((heads, SIDE, share, width), bf16),
            pltpu.VMEM((heads, SIDE, 8, 128), f32),
            pltpu.VMEM(out_weight.shape, bf16),
            pltpu.VMEM((share, depth), bf16),
            pltpu.VMEM((share, depth), bf16),
            dma(()),
            *attend_scratch,
            *ff_scratch,
        ],
        compiler_params=pltpu.CompilerParams(
            has_side_effects=True, collective_id=0, vmem_limit_bytes=VMEM
        ),
        name="layer",
    )(queries, keys, values, bias_rows, weights, residual, out_weight, gain, conv_gate, conv_value)[0]


def local(
    queries,
    keys,
    values,
    stick_bias,
    residual,
    out_weight,
    norm_gain,
    gate_weight,
    value_weight,
    down_weight,
    conv_gate,
    conv_value,
):
    rows_here = queries.shape[0]
    bias_rows = stick_bias.reshape(rows_here // CHUNK, CHUNK)
    bias_rows = jnp.pad(bias_rows, ((0, PAD - bias_rows.shape[0]), (0, 0)))
    weights = jnp.concatenate([gate_weight.T, value_weight.T, down_weight.T], axis=0)
    return layer(
        queries,
        keys,
        values,
        bias_rows,
        weights,
        residual,
        out_weight,
        norm_gain.reshape(1, -1),
        conv_gate,
        conv_value,
    )


def solution(mesh):
    in_specs = (
        P("sp", "tp"),
        P("sp", "tp"),
        P("sp", "tp"),
        P("sp", "tp"),
        P(("sp", "tp"), None),
        P(),
        P(),
        P("sp", "tp"),
        P("sp", "tp"),
        P("sp", "tp"),
        P(None, "tp"),
        P(None, "tp"),
    )
    out_specs = P(("sp", "tp"), None)
    return jax.shard_map(local, mesh=mesh, in_specs=in_specs, out_specs=out_specs, check_vma=False)
```

```python
import jax
import jax.numpy as jnp
from jax import lax
from jax.experimental import pallas as pl
from jax.experimental.pallas import tpu as pltpu
from jax.sharding import PartitionSpec as P

EPS = 1e-06
LOG2E = 1.4426950408889634
NT = (((1,), (1,)), ((), ()))
CHUNK = 256
PAD = 16
SIDE = 4
RIM = 16
VMEM = 67_000_000
ATTEND = 28
STAGES = (
    (0, 0, 3), (2, 0, 4), (4, 0, 5), (5, 0, 6), (7, 0, 7), (9, 0, 8), (11, 1, 0), (11, 1, 1),
)


def tri_matrix():
    rows = lax.broadcasted_iota(jnp.int32, (CHUNK, CHUNK), 0)
    cols = lax.broadcasted_iota(jnp.int32, (CHUNK, CHUNK), 1)
    return (rows > cols).astype(jnp.bfloat16), rows > cols


def visit_chunk(q, k, v, bias, tri, gone, acc, mask=None):
    scale = 128 ** (-0.5) * LOG2E
    s = lax.dot_general(q, k, NT, preferred_element_type=jnp.float32) * scale + bias
    if mask is not None:
        s = jnp.where(mask, s, -1e30)
    soft = jnp.maximum(jnp.log(1.0 + jnp.exp2(jnp.minimum(s, 126.0))) * LOG2E, s)
    behind = jnp.dot(soft.astype(jnp.bfloat16), tri, preferred_element_type=jnp.float32)
    stick = jnp.exp2((s - soft) - (behind + gone)).astype(jnp.bfloat16)
    acc = acc + jnp.dot(stick, v, preferred_element_type=jnp.float32)
    gone = gone + (behind[:, 0:1] + soft[:, 0:1])
    return gone, acc


def position():
    me = lax.axis_index("sp")
    return me, me // SIDE, me % SIDE


def owners_of(y):
    core = lax.axis_index("tp") % 2
    return 2 * ((y + core) % SIDE), 2 * ((y + core + 2) % SIDE) + 1


def place_of():
    me = lax.axis_index("tp")
    return me // 2, me % 2


def remote_copy(src, dst, send_sem, recv_sem, **where):
    return pltpu.make_async_remote_copy(
        src_ref=src,
        dst_ref=dst,
        send_sem=send_sem,
        recv_sem=recv_sem,
        device_id=where,
        device_id_type=pl.DeviceIdType.MESH,
    )


def arrived(dst, sem):
    pltpu.make_async_copy(dst, dst, sem).wait()


def meet(peers, extra=0):
    barrier = pltpu.get_barrier_semaphore()
    for where in peers:
        pl.semaphore_signal(barrier, inc=1, device_id=where, device_id_type=pl.DeviceIdType.MESH)
    pl.semaphore_wait(barrier, len(peers) + extra)


def attend_part(
    q_ref, k_ref, v_ref, b_ref, w_ref, os_ref, gs_ref, whole_ref,
    q_all, k_all, v_all, b_all, o_buf, g_buf, acc_ref, gone_ref, block_out, block_gone,
    kv_send, kv_recv, kv_own, bias_send, bias_recv, bias_own, q_send, q_recv, q_own, z_send, z_recv,
    w1_send, w1_relay, w2_send, w2_relay, w_recv, o_send, o_recv,
):
    me, z, y = position()
    x, core = place_of()
    head = lax.axis_index("tp")
    rows, width = k_ref.shape
    quarter = rows // SIDE
    share = quarter // 2
    chunks = rows // CHUNK
    right = (y + 1) % SIDE
    left = (y + 3) % SIDE
    across = (y + 2) % SIDE
    row = z * SIDE
    owners = owners_of(y)
    tri, _ = tri_matrix()

    barrier = pltpu.get_barrier_semaphore()

    def greet(group, carry):
        for source in range(os_ref.shape[0]):
            of = (x - source % 2 - 2 * core + 2 * SIDE) % SIDE
            pl.semaphore_signal(
                barrier,
                inc=1,
                device_id={"sp": group * SIDE + of, "tp": source},
                device_id_type=pl.DeviceIdType.MESH,
            )
        return carry

    lax.fori_loop(0, z + 1, greet, 0)

    @pl.when(me > 0)
    def _():
        pl.semaphore_signal(
            barrier,
            inc=1,
            device_id={"sp": me - 1, "tp": 2 * SIDE - 1},
            device_id_type=pl.DeviceIdType.MESH,
        )

    meet(
        [{"sp": row + (y + d) % SIDE} for d in (1, 2, 3)]
        + [{"sp": (z + d) % SIDE * SIDE + y} for d in (1, 2, 3)]
        + [{"tp": 2 * ((x + d) % SIDE) + core} for d in (1, 3)]
        + [{"tp": 2 * x + 1 - core}],
        2 * (SIDE * SIDE - row)
        + jnp.where((head == 2 * SIDE - 1) & (me < SIDE * SIDE - 1), 2 * SIDE, 0),
    )

    def hop(part, src_slot, to, lane):
        src = (k_ref, v_ref)[part] if src_slot is None else (k_all, v_all)[part].at[src_slot]
        slot = y if src_slot is None else src_slot
        return remote_copy(
            src,
            (k_all, v_all)[part].at[slot],
            kv_send.at[part, lane],
            kv_recv.at[part, slot],
            sp=row + to,
        )

    def kv_mine(part):
        return pltpu.make_async_copy(
            (k_ref, v_ref)[part], (k_all, v_all)[part].at[y], kv_own.at[part]
        )

    def bias_hop(d):
        return remote_copy(
            b_ref, b_all.at[y], bias_send.at[d], bias_recv.at[y], sp=row + (y + d) % SIDE
        )

    def q_source(of, half):
        return q_ref.at[pl.ds(pl.multiple_of(owners_of(of)[half] * share, share), share)]

    def q_mine(half):
        return pltpu.make_async_copy(
            q_source(y, half), q_all.at[me, pl.ds(half * share, share)], q_own.at[half]
        )

    def q_piece(d, half):
        of = (y + d) % SIDE
        return remote_copy(
            q_source(of, half),
            q_all.at[me, pl.ds(half * share, share)],
            q_send.at[d, half],
            q_recv.at[y, half],
            sp=row + of,
        )

    def q_down(dz):
        ours = q_all.at[pl.ds(pl.multiple_of(row, SIDE), SIDE)]
        return remote_copy(ours, ours, z_send.at[dz], z_recv.at[z], sp=row - dz * SIDE + y)

    third = w_ref.shape[0] // 3
    starts = (0, 2 * third)
    bulks = (third, third // 2)
    steps = (0, 3, 1, 2)

    def w_axes(part):
        return (y, z) if part == 0 else (z, y)

    def w_index(part, c1, c2):
        return c2 * SIDE + c1 if part == 0 else c1 * SIDE + c2

    def w_rows(batch, part, half):
        piece = bulks[batch] // 2
        return pl.ds(starts[batch] + (2 * part + half) * piece, piece)

    def w_copy(batch, part, half, c1, c2, own, to1, to2, send):
        slot = w_index(part, c1, c2)
        spot = whole_ref.at[slot, w_rows(batch, part, half)]
        src = w_ref.at[w_rows(batch, part, half)] if own else spot
        return remote_copy(
            src, spot, send, w_recv.at[batch, part, slot, half], sp=w_index(part, to1, to2)
        )

    def w_first(batch, part, way, half):
        c1, c2 = w_axes(part)
        to = (c1 + (1, 3)[way]) % SIDE
        return w_copy(batch, part, half, c1, c2, True, to, c2, w1_send.at[batch, part, way, half])

    def w_first_relay(batch, part, way):
        c1, c2 = w_axes(part)
        source = (c1 + (3, 1)[way]) % SIDE
        to = (c1 + (1, 3)[way]) % SIDE
        return w_copy(batch, part, way, source, c2, False, to, c2, w1_relay.at[batch, part, way])

    def w_second(batch, part, k, way, half):
        c1, c2 = w_axes(part)
        to = (c2 + (1, 3)[way]) % SIDE
        source = (c1 + steps[k]) % SIDE
        return w_copy(batch, part, half, source, c2, k == 0, c1, to, w2_send.at[batch, part, k, way, half])

    def w_second_relay(batch, part, k, way):
        c1, c2 = w_axes(part)
        source = (c2 + (3, 1)[way]) % SIDE
        to = (c2 + (1, 3)[way]) % SIDE
        return w_copy(
            batch, part, way, (c1 + steps[k]) % SIDE, source, False, c1, to, w2_relay.at[batch, part, k, way]
        )

    def w_take(batch, part, half, c1, c2):
        slot = w_index(part, c1, c2)
        arrived(whole_ref.at[slot, w_rows(batch, part, half)], w_recv.at[batch, part, slot, half])

    def w_near(part):
        c1, c2 = w_axes(part)
        return (c1 + 3) % SIDE, (c1 + 1) % SIDE, (c1 + 2) % SIDE, c2

    def w_own(batch, first_part):
        for half in range(2):
            for way in range(2):
                of = (half + way) % 2
                w_first(batch, first_part, way, of).start()
                w_second(batch, 1 - first_part, 0, way, of).start()

    def w_stage(batch, stage):
        if stage == 0:
            w_own(batch, 0)
        elif stage == 1:
            w_own(batch, 1)
        elif stage == 2:
            for way in range(2):
                for part in (1, 0):
                    near = w_near(part)
                    w_take(batch, part, way, near[way], near[3])
                    w_first_relay(batch, part, way).start()
        elif stage == 3:
            for part in (1, 0):
                near = w_near(part)
                for way in range(2):
                    w_take(batch, part, 1 - way, near[way], near[3])
            for half in range(2):
                for k in (1, 2):
                    for way in range(2):
                        for part in (1, 0):
                            w_second(batch, part, k, way, (half + way) % 2).start()
        elif stage == 4:
            for part in (1, 0):
                near = w_near(part)
                for half in range(2):
                    w_take(batch, part, half, near[2], near[3])
            for half in range(2):
                for way in range(2):
                    for part in (1, 0):
                        w_second(batch, part, 3, way, (half + way) % 2).start()
        elif stage < 9:
            k = stage - 5
            for way in range(2):
                for part in (1, 0):
                    c1, c2 = w_axes(part)
                    w_take(batch, part, way, (c1 + steps[k]) % SIDE, (c2 + (3, 1)[way]) % SIDE)
                    w_second_relay(batch, part, k, way).start()
        else:
            for part in range(2):
                c1, c2 = w_axes(part)
                for k in range(SIDE):
                    source = (c1 + steps[k]) % SIDE
                    w_take(batch, part, 1, source, (c2 + 3) % SIDE)
                    w_take(batch, part, 0, source, (c2 + 1) % SIDE)
                    for half in range(2):
                        w_take(batch, part, half, source, (c2 + 2) % SIDE)

    def w_sent():
        for batch in range(2):
            for part in range(2):
                for way in range(2):
                    w_first_relay(batch, part, way).wait_send()
                    for half in range(2):
                        w_first(batch, part, way, half).wait_send()
                    for k in range(SIDE):
                        w_second_relay(batch, part, k, way).wait_send()
                        for half in range(2):
                            w_second(batch, part, k, way, half).wait_send()

    def out_pieces(block, half):
        src = o_buf.at[block, pl.ds(half * share, share)]
        return ((src, os_ref), (g_buf.at[block, half], gs_ref))

    def out_remote(block, half, part):
        src, dst = out_pieces(block, half)[part]
        return remote_copy(
            src,
            dst.at[head, z],
            o_send.at[part, block, half],
            o_recv.at[part, head, z],
            sp=block,
            tp=owners[half],
        )

    def out_local(block, half, part):
        src, dst = out_pieces(block, half)[part]
        return pltpu.make_async_copy(src, dst.at[head, z], o_recv.at[part, head, z])

    def for_outs(group, act, act_local):
        for m in range(SIDE):
            block = group * SIDE + m
            for half in range(2):
                mine = (block == me) & (owners[half] == head)
                if act_local is not None:

                    @pl.when(mine)
                    def _():
                        for part in range(2):
                            act_local(out_local(block, half, part))

                @pl.when(jnp.logical_not(mine))
                def _():
                    for part in range(2):
                        act(out_remote(block, half, part))

    def finish(group):
        acc = acc_ref[...]
        gone = gone_ref[...]
        for m in range(SIDE):
            here = slice(m * quarter, (m + 1) * quarter)
            o_buf[group * SIDE + m] = acc[here].astype(o_buf.dtype)
            turned = gone[here].T
            for half in range(2):
                g_buf[group * SIDE + m, half] = turned[0:8, half * 128 : (half + 1) * 128]
        for_outs(group, lambda copy: copy.start(), lambda copy: copy.start())

    w_stage(0, 1)
    for half in range(2):
        q_mine(half).start()
    for d in (2, 1, 3):
        for half in range(2):
            q_piece(d, half).start()
        bias_hop(d).start()
    hop(0, None, right, 0).start()
    hop(1, None, left, 0).start()
    hop(1, None, right, 1).start()
    hop(0, None, left, 1).start()
    for part in range(2):
        kv_mine(part).start()
    bias_mine = pltpu.make_async_copy(b_ref, b_all.at[y], bias_own)
    bias_mine.start()

    first, second = (owner * share for owner in owners)
    at_row = lax.broadcasted_iota(jnp.int32, (rows, CHUNK), 0)
    col = lax.broadcasted_iota(jnp.int32, (rows, CHUNK), 1)
    inside = at_row % quarter
    place = (
        at_row // quarter * rows
        + inside
        + jnp.where(inside < share, first, second - share)
        - col
    )

    def diagonal(i, carry):
        j = (y + jnp.where(i == 0, 0, jnp.where(i == 1, 3, i - 1))) % SIDE

        @pl.when(i == 0)
        def _():
            for half in range(2):
                q_mine(half).wait()
                for d in (1, 2, 3):
                    slot = (y + d) % SIDE
                    arrived(q_all.at[row + slot, pl.ds(half * share, share)], q_recv.at[slot, half])
            for dz in (2, 3, 1):

                @pl.when(z >= dz)
                def _():
                    q_down(dz).start()

            for part in range(2):
                kv_mine(part).wait()
            bias_mine.wait()

        @pl.when(i == 1)
        def _():
            arrived(k_all.at[left], kv_recv.at[0, left])
            hop(0, left, right, 2).start()
            arrived(v_all.at[right], kv_recv.at[1, right])
            hop(1, right, left, 2).start()
            w_stage(0, 0)
            arrived(v_all.at[left], kv_recv.at[1, left])
            arrived(b_all.at[left], bias_recv.at[left])

        @pl.when(i == 2)
        def _():
            arrived(k_all.at[right], kv_recv.at[0, right])
            arrived(b_all.at[right], bias_recv.at[right])

        @pl.when(i == 3)
        def _():
            arrived(k_all.at[across], kv_recv.at[0, across])
            arrived(v_all.at[across], kv_recv.at[1, across])
            arrived(b_all.at[across], bias_recv.at[across])

        q = q_all[pl.ds(row, SIDE)].reshape(rows, width)
        bias = b_all[j].astype(jnp.float32) * LOG2E
        gone = jnp.zeros((rows, 1), jnp.float32)
        acc = jnp.zeros((rows, width), jnp.float32)
        for c in range(chunks - 1, -1, -1):
            at = slice(c * CHUNK, (c + 1) * CHUNK)
            mask = place > j * rows + c * CHUNK
            gone, acc = visit_chunk(
                q, k_all[j, at, :], v_all[j, at, :], bias[c : c + 1, :], tri, gone, acc, mask
            )
        block_out[j] = acc
        block_gone[j] = jnp.broadcast_to(gone, (rows, 128))
        return carry

    lax.fori_loop(0, SIDE, diagonal, 0)
    gone = block_gone[SIDE - 1]
    acc = block_out[SIDE - 1]
    for j in range(SIDE - 2, -1, -1):
        acc = acc + jnp.exp2(-gone) * block_out[j]
        gone = gone + block_gone[j]
    acc_ref[...] = acc
    gone_ref[...] = gone
    finish(z)
    w_stage(0, 2)
    for other in range(1, SIDE):

        @pl.when(z < other)
        def _():
            arrived(q_all.at[pl.ds(other * SIDE, SIDE)], z_recv.at[other])

    def step(s, carry):
        group = z + 1 + s // SIDE
        j = SIDE - 1 - s % SIDE

        @pl.when(group < SIDE)
        def _():
            @pl.when(j == SIDE - 1)
            def _():
                acc_ref[...] = jnp.zeros_like(acc_ref)
                gone_ref[...] = jnp.zeros_like(gone_ref)

            q = q_all[pl.ds(group * SIDE, SIDE)].reshape(rows, width)
            bias = b_all[j].astype(jnp.float32) * LOG2E
            gone = gone_ref[:, 0:1]
            acc = acc_ref[...]
            for c in range(chunks - 1, -1, -1):
                at = slice(c * CHUNK, (c + 1) * CHUNK)
                gone, acc = visit_chunk(
                    q, k_all[j, at, :], v_all[j, at, :], bias[c : c + 1, :], tri, gone, acc
                )
            acc_ref[...] = acc
            gone_ref[...] = jnp.broadcast_to(gone, (rows, 128))

            @pl.when(j == 0)
            def _():
                finish(group)

        for after, batch, stage in STAGES:

            @pl.when(s == after)
            def _():
                w_stage(batch, stage)

        return carry

    lax.fori_loop(0, (SIDE - 1) * SIDE, step, 0)

    def take(group, carry):
        for h in range(os_ref.shape[0]):
            for part in range(2):
                arrived((os_ref, gs_ref)[part].at[h, group], o_recv.at[part, h, group])
        return carry

    lax.fori_loop(0, z + 1, take, 0)
    def up_weights():
        w_stage(0, 9)

    def down_weights(stage):
        w_stage(1, stage)

    def all_sent():
        def sent(group, carry):
            for_outs(group, lambda copy: copy.wait_send(), None)
            return carry

        lax.fori_loop(z, SIDE, sent, 0)
        w_sent()
        hop(0, None, right, 0).wait_send()
        hop(1, None, left, 0).wait_send()
        hop(1, None, right, 1).wait_send()
        hop(0, None, left, 1).wait_send()
        hop(0, left, right, 2).wait_send()
        hop(1, right, left, 2).wait_send()
        for d in (1, 2, 3):
            bias_hop(d).wait_send()
            for half in range(2):
                q_piece(d, half).wait_send()
        for dz in (1, 2, 3):

            @pl.when(z >= dz)
            def _():
                q_down(dz).wait_send()

    return up_weights, down_weights, all_sent


def feed_forward_part(
    up_weights, down_weights, n_ref, m_ref, mine_ref, w_ref, cg_ref, cv_ref, out_ref,
    all_ref, rim_ref, up_ref, down_ref, gate_ref, value_ref, p_ref, twin_buf, sum_buf, relay_buf,
    ring_buf, w_sem, ring_send, ring_recv, twin_send, twin_recv, rim_send, rim_recv, own_sem,
    pair_send, pair_recv, relay_send, relay_recv, back_send, back_recv,
):
    x, core = place_of()
    block = lax.axis_index("sp")
    rows, depth = n_ref.shape
    part = rows // 2
    tile = 2 * rows
    units = down_ref.shape[0]
    shards = w_ref.shape[0]
    deep = depth // shards
    right = (x + 1) % SIDE
    left = (x + 3) % SIDE
    across = (x + 2) % SIDE
    other = 2 * x + 1 - core
    halves = (slice(0, part), slice(part, rows))

    def up_copy(k, src):
        at = slice(k * deep, (k + 1) * deep)
        return pltpu.make_async_copy(src.at[pl.ds(0, 2 * units)], up_ref.at[:, at], w_sem.at[0, k])

    def down_copy(k, src):
        at = slice(k * deep, (k + 1) * deep)
        return pltpu.make_async_copy(
            src.at[pl.ds(2 * units, units)], down_ref.at[:, at], w_sem.at[1, k]
        )

    def load(copy):
        for k in range(shards):

            @pl.when(block == k)
            def _():
                copy(k, mine_ref).start()

            @pl.when(block != k)
            def _():
                copy(k, w_ref.at[k]).start()

    def spot(chip, half, of_core):
        return all_ref.at[2 * chip + of_core, pl.ds(half * part, part)]

    def ring(chip, half, to, lane):
        src = n_ref.at[pl.ds(half * part, part)] if chip is None else spot(chip, half, core)
        chip = x if chip is None else chip
        return remote_copy(
            src,
            spot(chip, half, core),
            ring_send.at[lane, half],
            ring_recv.at[chip, half],
            tp=2 * to + core,
        )

    def twin(chip, half):
        src = n_ref.at[pl.ds(half * part, part)] if chip is None else spot(chip, half, core)
        chip = x if chip is None else chip
        return remote_copy(
            src, spot(chip, half, core), twin_send.at[chip, half], twin_recv.at[chip, half], tp=other
        )

    def rim(to):
        return remote_copy(
            n_ref.at[pl.ds(rows - RIM, RIM)], rim_ref, rim_send.at[to], rim_recv, sp=block + 1, tp=to
        )

    last = (x == SIDE - 1) & (core == 1) & (block < SIDE * SIDE - 1)
    own = pltpu.make_async_copy(n_ref, all_ref.at[2 * x + core], own_sem)
    ring(None, 0, right, 0).start()
    ring(None, 1, left, 1).start()
    ring(None, 1, right, 0).start()
    ring(None, 0, left, 1).start()
    own.start()
    for half in range(2):
        twin(None, half).start()

    @pl.when(last)
    def _():
        for to in range(2 * SIDE):
            rim(to).start()

    def up(rows_in, which):
        w = up_ref[which * units : (which + 1) * units, :]
        return lax.dot_general(rows_in, w, NT, preferred_element_type=jnp.float32)

    def project_up(chip):
        rows_in = all_ref[pl.ds(2 * chip, 2)].reshape(tile, depth)
        for which, ref in enumerate((gate_ref, value_ref)):
            ref[pl.ds(pl.multiple_of(chip * tile + RIM, RIM), tile), :] = up(rows_in, which)

    def conv(ref, taps, chip):
        window = ref[pl.ds(pl.multiple_of(chip * tile, tile), tile + RIM), :]
        return (
            taps[0:1, :] * window[RIM - 2 : RIM - 2 + tile]
            + taps[1:2, :] * window[RIM - 1 : RIM - 1 + tile]
            + taps[2:3, :] * window[RIM : RIM + tile]
        )

    def project_down(chip):
        gate = conv(gate_ref, cg_ref, chip)
        value = conv(value_ref, cv_ref, chip)
        hidden = (gate / (1.0 + jnp.exp(-gate)) * value).astype(jnp.bfloat16)
        down = jnp.dot(hidden, down_ref[...], preferred_element_type=jnp.float32)
        p_ref[pl.ds(2 * chip, 2)] = down.astype(p_ref.dtype).reshape(2, rows, depth)

    def twin_arrived(chip):
        for half in range(2):
            arrived(spot(chip, half, 1 - core), twin_recv.at[chip, half])

    up_weights()
    load(up_copy)
    down_weights(2)
    for k in range(shards):
        up_copy(k, mine_ref).wait()
    own.wait()
    twin_arrived(x)
    project_up(x)
    down_weights(3)
    arrived(spot(left, 0, core), ring_recv.at[left, 0])
    ring(left, 0, right, 2).start()
    twin(left, 0).start()
    arrived(spot(right, 1, core), ring_recv.at[right, 1])
    ring(right, 1, left, 2).start()
    twin(right, 1).start()

    down_weights(4)

    @pl.when(block > 0)
    def _():
        arrived(rim_ref, rim_recv)
        for which, ref in enumerate((gate_ref, value_ref)):
            ref[0:RIM, :] = up(rim_ref[...], which)

    @pl.when(block == 0)
    def _():
        for ref in (gate_ref, value_ref):
            ref[0:RIM, :] = jnp.zeros((RIM, units), jnp.float32)

    for chip, half in ((left, 1), (right, 0)):
        arrived(spot(chip, half, core), ring_recv.at[chip, half])
        twin(chip, half).start()
    down_weights(5)
    down_weights(6)
    twin_arrived(right)
    project_up(right)
    down_weights(7)
    down_weights(8)
    twin_arrived(left)
    project_up(left)
    down_weights(9)
    load(down_copy)
    for half in range(2):
        arrived(spot(across, half, core), ring_recv.at[across, half])
        twin(across, half).start()
    for k in range(shards):
        down_copy(k, mine_ref).wait()

    def pair(chip):
        return remote_copy(
            p_ref.at[2 * chip + 1 - core],
            twin_buf.at[chip],
            pair_send.at[chip],
            pair_recv.at[chip],
            tp=other,
        )

    def pair_sum(chip, half):
        mine = p_ref[2 * chip + core, halves[half], :].astype(jnp.float32)
        return mine + twin_buf[chip, halves[half], :].astype(jnp.float32)

    def relay(side):
        return remote_copy(
            sum_buf.at[0, halves[side]],
            relay_buf.at[side],
            relay_send.at[side],
            relay_recv.at[side],
            tp=2 * (right, left)[side] + core,
        )

    def back(side, half):
        return remote_copy(
            sum_buf.at[1 + side, halves[half]],
            ring_buf.at[side, halves[half]],
            back_send.at[side, half],
            back_recv.at[side, half],
            tp=2 * (right, left)[side] + core,
        )

    def direct(side):
        to = (right, left)[side]
        half = 1 - side
        arrived(twin_buf.at[to], pair_recv.at[to])
        sum_buf[1 + side, halves[half], :] = pair_sum(to, half).astype(jnp.bfloat16)
        back(side, half).start()

    project_down(right)
    pair(right).start()
    twin_arrived(across)
    direct(0)
    project_up(across)
    project_down(across)
    pair(across).start()
    arrived(twin_buf.at[across], pair_recv.at[across])
    for side in range(2):
        sum_buf[0, halves[side], :] = pair_sum(across, side).astype(jnp.bfloat16)
        relay(side).start()
    project_down(left)
    pair(left).start()
    direct(1)
    project_down(x)
    pair(x).start()
    for side in range(2):
        to = (right, left)[side]
        arrived(relay_buf.at[side], relay_recv.at[side])
        total = pair_sum(to, side) + relay_buf[side].astype(jnp.float32)
        sum_buf[1 + side, halves[side], :] = total.astype(jnp.bfloat16)
        back(side, side).start()
    arrived(twin_buf.at[x], pair_recv.at[x])
    for half in range(2):
        total = m_ref[halves[half], :].astype(jnp.float32) + pair_sum(x, half)
        for side in (1 - half, half):
            arrived(ring_buf.at[side, halves[half]], back_recv.at[side, half])
            total = total + ring_buf[side, halves[half], :].astype(jnp.float32)
        out_ref[halves[half], :] = total.astype(out_ref.dtype)

    for half in range(2):
        ring(None, half, right, 0).wait_send()
        ring(None, half, left, 1).wait_send()
        twin(None, half).wait_send()
        for chip in (left, right, across):
            twin(chip, half).wait_send()
    ring(left, 0, right, 2).wait_send()
    ring(right, 1, left, 2).wait_send()

    @pl.when(last)
    def _():
        for to in range(2 * SIDE):
            rim(to).wait_send()

    for chip in range(SIDE):
        pair(chip).wait_send()
    for side in range(2):
        relay(side).wait_send()
        for half in range(2):
            back(side, half).wait_send()


def middle_part(os_ref, gs_ref, res_ref, ow_ref, gain_ref, m_ref, n_ref):
    z = position()[1]
    heads, groups, rows, width = os_ref.shape
    outs = [jnp.zeros((rows, width), jnp.float32) for _ in range(heads)]
    later = jnp.zeros((rows, 128), jnp.float32)
    for group in range(groups - 1, -1, -1):
        valid = group <= z
        weight = jnp.exp2(-later)
        for h in range(heads):
            term = jnp.where(valid, os_ref[h, group].astype(jnp.float32), 0.0)
            outs[h] = outs[h] + term * weight[:, h : h + 1]
        if group:
            left = jnp.concatenate([gs_ref[h, group, 0:1, :] for h in range(heads)], axis=0)
            left = jnp.where(valid, left, 0.0)
            later = later + jnp.concatenate([left] * (128 // heads), axis=0).T
    attended = jnp.concatenate(outs, axis=1).astype(jnp.bfloat16)
    projected = jnp.dot(attended, ow_ref[...], preferred_element_type=jnp.float32)
    middle = (res_ref[...].astype(jnp.float32) + projected).astype(jnp.bfloat16)
    m_ref[...] = middle
    wide = middle.astype(jnp.float32)
    scale = lax.rsqrt(jnp.mean(wide * wide, axis=-1, keepdims=True) + EPS)
    n_ref[...] = (wide * scale * gain_ref[...]).astype(jnp.bfloat16)


def layer_kernel(*refs):
    q, k, v, b, w, res, ow, gain, cg, cv, out, whole = refs[:12]
    os_ref, gs_ref, ow_ref, m_ref, n_ref, ow_sem = refs[12:18]
    attend_refs = refs[18 : 18 + ATTEND]
    ff_refs = refs[18 + ATTEND :]
    ow_copy = pltpu.make_async_copy(ow, ow_ref, ow_sem)
    ow_copy.start()
    up_weights, down_weights, all_sent = attend_part(q, k, v, b, w, os_ref, gs_ref, whole, *attend_refs)
    ow_copy.wait()
    middle_part(os_ref, gs_ref, res, ow_ref, gain, m_ref, n_ref)
    feed_forward_part(up_weights, down_weights, n_ref, m_ref, w, whole, cg, cv, out, *ff_refs)
    all_sent()


def layer(queries, keys, values, bias_rows, weights, residual, out_weight, gain, conv_gate, conv_value):
    rows, width = queries.shape
    share, depth = residual.shape
    units = conv_gate.shape[1]
    heads = lax.axis_size("tp")
    count = SIDE * SIDE
    quarter = rows // SIDE
    anywhere = pl.BlockSpec(memory_space=pl.ANY)
    vmem = pl.BlockSpec(memory_space=pltpu.VMEM)
    dma = pltpu.SemaphoreType.DMA
    bf16 = jnp.bfloat16
    f32 = jnp.float32
    attend_scratch = [
        pltpu.VMEM((count, quarter, width), bf16),
        pltpu.VMEM((SIDE, rows, width), bf16),
        pltpu.VMEM((SIDE, rows, width), bf16),
        pltpu.VMEM((SIDE,) + bias_rows.shape, bf16),
        pltpu.VMEM((count, quarter, width), bf16),
        pltpu.VMEM((count, 2, 8, 128), f32),
        pltpu.VMEM((rows, width), f32),
        pltpu.VMEM((rows, 128), f32),
        pltpu.VMEM((SIDE, rows, width), f32),
        pltpu.VMEM((SIDE, rows, 128), f32),
        dma((2, 3)), dma((2, SIDE)), dma((2,)), dma((SIDE,)), dma((SIDE,)), dma(()),
        dma((SIDE, 2)), dma((SIDE, 2)), dma((2,)), dma((SIDE,)), dma((SIDE,)),
        dma((2, 2, 2, 2)), dma((2, 2, 2)), dma((2, 2, SIDE, 2, 2)), dma((2, 2, SIDE, 2)),
        dma((2, 2, count, 2)), dma((2, count, 2)), dma((2, heads, SIDE)),
    ]
    ff_scratch = [
        pltpu.VMEM((2 * SIDE, share, depth), bf16),
        pltpu.VMEM((RIM, depth), bf16),
        pltpu.VMEM((2 * units, depth), bf16),
        pltpu.VMEM((units, depth), bf16),
        pltpu.VMEM((RIM + rows, units), f32),
        pltpu.VMEM((RIM + rows, units), f32),
        pltpu.VMEM((2 * SIDE, share, depth), bf16),
        pltpu.VMEM((SIDE, share, depth), bf16),
        pltpu.VMEM((3, share, depth), bf16),
        pltpu.VMEM((2, share // 2, depth), bf16),
        pltpu.VMEM((2, share, depth), bf16),
        dma((2, count)),
        dma((3, 2)), dma((SIDE, 2)), dma((SIDE, 2)), dma((SIDE, 2)), dma((2 * SIDE,)), dma(()), dma(()),
        dma((SIDE,)), dma((SIDE,)), dma((2,)), dma((2,)), dma((2, 2)), dma((2, 2)),
    ]
    assert len(attend_scratch) == ATTEND
    return pl.pallas_call(
        layer_kernel,
        out_shape=(
            jax.ShapeDtypeStruct((share, depth), bf16),
            jax.ShapeDtypeStruct((count,) + weights.shape, bf16),
        ),
        in_specs=[anywhere, anywhere, anywhere, vmem, anywhere, vmem, anywhere, vmem, vmem, vmem],
        out_specs=[vmem, anywhere],
        scratch_shapes=[
            pltpu.VMEM((heads, SIDE, share, width), bf16),
            pltpu.VMEM((heads, SIDE, 8, 128), f32),
            pltpu.VMEM(out_weight.shape, bf16),
            pltpu.VMEM((share, depth), bf16),
            pltpu.VMEM((share, depth), bf16),
            dma(()),
            *attend_scratch,
            *ff_scratch,
        ],
        compiler_params=pltpu.CompilerParams(
            has_side_effects=True, collective_id=0, vmem_limit_bytes=VMEM
        ),
        name="layer",
    )(queries, keys, values, bias_rows, weights, residual, out_weight, gain, conv_gate, conv_value)[0]


def local(
    queries,
    keys,
    values,
    stick_bias,
    residual,
    out_weight,
    norm_gain,
    gate_weight,
    value_weight,
    down_weight,
    conv_gate,
    conv_value,
):
    rows_here = queries.shape[0]
    bias_rows = stick_bias.reshape(rows_here // CHUNK, CHUNK)
    bias_rows = jnp.pad(bias_rows, ((0, PAD - bias_rows.shape[0]), (0, 0)))
    weights = jnp.concatenate([gate_weight.T, value_weight.T, down_weight.T], axis=0)
    return layer(
        queries,
        keys,
        values,
        bias_rows,
        weights,
        residual,
        out_weight,
        norm_gain.reshape(1, -1),
        conv_gate,
        conv_value,
    )


def solution(mesh):
    in_specs = (
        P("sp", "tp"),
        P("sp", "tp"),
        P("sp", "tp"),
        P("sp", "tp"),
        P(("sp", "tp"), None),
        P(),
        P(),
        P("sp", "tp"),
        P("sp", "tp"),
        P("sp", "tp"),
        P(None, "tp"),
        P(None, "tp"),
    )
    out_specs = P(("sp", "tp"), None)
    return jax.shard_map(local, mesh=mesh, in_specs=in_specs, out_specs=out_specs, check_vma=False)
```
